256 devices in a mesh: sp: 64 (over z, y, core), tp: 4 (over x).
Axes of the slice: x: 4, y: 4, z: 8, core: 2. Of those that a mesh axis runs over, the one named last changes fastest.
Arguments:
- queries: bfloat16 [16384, 2048], P('sp', 'tp'), may hold values from -16 to 16
- key_value_pairs: bfloat16 [16384, 512], P('sp', 'tp'), may hold values from -16 to 16
- forget_gate_total: float32 [16384, 32], P('sp', 'tp'), may hold values from -16384 to 0, as said below
- residual_in: bfloat16 [16384, 2048], P(('sp', 'tp')), may hold values from -12 to 12
- out_weight: bfloat16 [2048, 2048], P('tp'), may hold values from -0.25 to 0.25
- norm_gain: float32 [2048], replicated, may hold values from 0.1 to 1.9
- routes: int32 [16384, 2], P(('sp', 'tp')), may hold values from 0 to 63, all different within a row; in each aligned block of 64 rows (0 to 63, 64 to 127, ...) at most 3 rows name the same one
- route_weight: float32 [16384, 2], P(('sp', 'tp')), may hold values from 0.2 to 1
- expert_gate: bfloat16 [64, 2048, 3072], P('sp', None, 'tp'), may hold values from -0.125 to 0.125
- expert_up: bfloat16 [64, 2048, 3072], P('sp', None, 'tp'), may hold values from -0.125 to 0.125
- expert_down: bfloat16 [64, 3072, 2048], P('sp', 'tp'), may hold values from -0.109375 to 0.109375
Outputs:
- layer_out: bfloat16 [16384, 2048], P(('sp', 'tp'))
The draws below stay inside these ranges and needn't reach their ends.
Inputs may be any that keep to these rules, and one draw needn't show every extreme that they name: `routes`: each row names 2 different experts; among the rows of one device no expert is named more than 3 times, and in every draw some device names some expert exactly 3 times. `forget_gate_total`: along the positions, each head's values never rise.
All inputs are finite; a program needn't handle non-finite values.
Results may differ from the reference program's by a relative error of at most 0.011.
Values may be sent and summed in bfloat16 or wider, within the bound.
No kernel may reach another device: no remote copies, remote signals or barrier semaphores. Data moves between devices by JAX's collectives and lax.ppermute only.
A program may use at most 64 MiB of HBM per device.

```python
import math
import jax
import jax.numpy as jnp
import numpy as np
from jax import lax

D = 2048
QUERY_HEADS = 32
KEY_VALUE_HEADS = 4
HEAD_SIZE = 64
FF = 3072
TOP = 2
TOK_DEV = 256
SEQUENCE_TOKENS = 16384
ROWS_DEV = 64
EXPERTS = 64
CAPACITY = 3
N_SP = 64
N_TP = 4


def draw_queries(key, part):
    array_shape = (SEQUENCE_TOKENS, QUERY_HEADS * HEAD_SIZE)
    base = jax.random.normal(jax.random.fold_in(key, 1), array_shape, jnp.float32)
    return jnp.clip(1.4 * base, -5.6, 5.6).astype(jnp.bfloat16)


def draw_key_value_pairs(key, part):
    array_shape = (SEQUENCE_TOKENS, KEY_VALUE_HEADS, HEAD_SIZE)
    key_portion = jnp.clip(1.4 * jax.random.normal(jax.random.fold_in(key, 2), array_shape, jnp.float32), -5.6, 5.6)
    value_portion = jnp.clip(jax.random.normal(jax.random.fold_in(key, 3), array_shape, jnp.float32), -4.0, 4.0)
    return jnp.concatenate([key_portion, value_portion], axis=2).reshape(SEQUENCE_TOKENS, KEY_VALUE_HEADS * 2 * HEAD_SIZE).astype(jnp.bfloat16)


def draw_forget_gate_total(key, part):
    order = jax.random.permutation(jax.random.fold_in(key, 21), QUERY_HEADS)
    fast = order < QUERY_HEADS // 2
    slow_total = jnp.exp(jax.random.uniform(jax.random.fold_in(key, 22), (QUERY_HEADS,), jnp.float32, math.log(0.2), math.log(0.8)))
    fast_rate = jnp.exp(jax.random.uniform(jax.random.fold_in(key, 23), (QUERY_HEADS,), jnp.float32, math.log(0.03), math.log(0.1)))
    rate = jnp.where(fast, fast_rate, slow_total / SEQUENCE_TOKENS)
    blocks = SEQUENCE_TOKENS // TOK_DEV
    block_factor = jnp.exp(jax.random.uniform(jax.random.fold_in(key, 24), (blocks, QUERY_HEADS), jnp.float32, math.log(0.5), math.log(2.0)))
    rough = jax.random.uniform(jax.random.fold_in(key, 25), (SEQUENCE_TOKENS, QUERY_HEADS), jnp.float32, 0.3, 1.7)
    loop_steps = rate[None, :] * jnp.repeat(block_factor, TOK_DEV, axis=0) * rough
    segment_begin = jax.random.randint(jax.random.fold_in(key, 26), (2,), 0, SEQUENCE_TOKENS)
    segment_length = jax.random.uniform(jax.random.fold_in(key, 27), (2, QUERY_HEADS), jnp.float32, 0.2, 0.4)
    segment_list = jnp.zeros((SEQUENCE_TOKENS, QUERY_HEADS), jnp.float32).at[segment_begin].add(-jnp.log(1.0 - segment_length))
    return -jnp.cumsum(loop_steps + segment_list, axis=0)


def draw_residual_in(key, part):
    base = jax.random.normal(jax.random.fold_in(key, 31), (SEQUENCE_TOKENS, D), jnp.float32)
    return jnp.clip(base, -6.0, 6.0).astype(jnp.bfloat16)


def levels(own_key, extent, split, least, top_value):
    def one(axis_at, shards_of):
        steps = jax.random.uniform(jax.random.fold_in(jax.random.fold_in(own_key, 6), axis_at), (shards_of,), jnp.float32, least / len(split), top_value / len(split))
        return jnp.repeat(jnp.exp(steps), extent[axis_at] // shards_of).reshape((-1,) + (1,) * (len(extent) - axis_at - 1))

    level = one(*split[0])
    for cut in split[1:]:
        level = level * one(*cut)
    return level


def assign_block(stream_key, own, number, rows, count, top, most, lean):
    order = jax.random.permutation(stream_key, count)
    packed, ordinary = shares(count, rows * top, most, lean, True), shares(count, rows * top, most, lean, False)
    places = jnp.arange(count)

    def named(sizes, rotation):
        used = int((sizes > 0).sum())
        fixed = max(1, used // 4)
        moved = fixed + (places - fixed + rotation * (used - fixed)) % max(1, count - fixed)
        return jnp.zeros((count,), jnp.int32).at[order[jnp.where(places < fixed, places, moved)]].set(jnp.asarray(sizes, jnp.int32))

    sizes = jnp.where(number % 4 == 0, named(packed, number // 4), named(ordinary, number - number // 4 - 1))
    mixed = jax.random.permutation(jax.random.fold_in(own, 3), count)
    source_of, receiver = mixed[0:count // 2 * 2:2], mixed[1:count // 2 * 2:2]
    slack = jnp.minimum(sizes[source_of] - 1, most - sizes[receiver]) // 2
    slack = jnp.where((source_of == order[0]) | (receiver == order[0]) | (sizes[receiver] == 0), 0, jnp.maximum(slack, 0))
    moved = jax.random.randint(jax.random.fold_in(own, 4), (count // 2,), 0, 1 << 20) % (slack + 1)
    sizes = sizes.at[source_of].add(-moved).at[receiver].add(moved)
    members = jnp.searchsorted(jnp.cumsum(sizes), jnp.arange(rows * top), side="right").astype(jnp.int32)
    grid = members.reshape(top, rows).T
    grid = grid[jax.random.permutation(jax.random.fold_in(own, 1), rows)]
    rotation = jax.random.randint(jax.random.fold_in(own, 2), (rows, 1), 0, top)
    return jnp.take_along_axis(grid, (jnp.arange(top)[None, :] + rotation) % top, axis=1)


def shares(count, total, most, slope, full):
    weights = [(1 << 20) // math.isqrt(rank ** slope) + 1 for rank in range(1, count + 1)]
    largest = most if full else min(most, max(-(-total // count), total * weights[0] // sum(weights)))
    least = 1 if total - largest >= count - 1 else 0
    holding, rest = [largest] + [least] * (count - 1), total - largest - least * (count - 1)
    while rest > 0:
        candidates = [i for i in range(1, count) if holding[i] < largest] or [i for i in range(1, count) if holding[i] < most]
        pool, left = sum([weights[i] for i in candidates]), rest
        for i in candidates:
            addition = min(most - holding[i], max(1, left * weights[i] // pool), rest)
            holding[i] = holding[i] + addition
            rest = rest - addition
    return np.array(holding)


def centred(own_key, shape, width, reach, split=(), held_as=jnp.bfloat16):
    values = jax.random.normal(own_key, shape, jnp.float32) * width
    if len(split) > 0:
        values = levels(own_key, shape, split, -0.22, 0.18) * values
    return jnp.clip(values, min=-reach, max=reach).astype(held_as)


def setup_inputs(seed: int = 0) -> dict:
    key_list = jax.random.split(jax.random.key(seed), 12)
    queries = draw_queries(jax.random.fold_in(key_list[11], 71), 0)
    key_value_pairs = draw_key_value_pairs(jax.random.fold_in(key_list[11], 71), 0)
    forget_gate_total = draw_forget_gate_total(jax.random.fold_in(key_list[11], 71), 0)
    residual_in = draw_residual_in(jax.random.fold_in(key_list[11], 71), 0)
    out_weight = centred(key_list[4], (QUERY_HEADS * HEAD_SIZE, D), (QUERY_HEADS * HEAD_SIZE // 4) ** -0.5, 0.25, ((0, 4),))
    norm_gain = jnp.clip(1.0 + 0.18 * jax.random.normal(key_list[5], (D,), jnp.float32), 0.1, 1.9)
    routes_keys = jax.random.split(jax.random.fold_in(key_list[6], 1), SEQUENCE_TOKENS // ROWS_DEV)
    routes_turns = jax.random.permutation(jax.random.fold_in(key_list[6], 3), SEQUENCE_TOKENS // ROWS_DEV)
    routes = jax.vmap(lambda own, number: assign_block(jax.random.fold_in(key_list[6], 2), own, number, ROWS_DEV, EXPERTS, TOP, CAPACITY, 2))(routes_keys, routes_turns).reshape((SEQUENCE_TOKENS, TOP))
    route_weight = jnp.clip(0.2 + 0.8 * jax.random.uniform(key_list[7], (SEQUENCE_TOKENS, TOP), jnp.float32) ** levels(key_list[7], (SEQUENCE_TOKENS, TOP), ((0, 256),), -0.2, 0.2), 0.2, 1.0)
    expert_gate = centred(key_list[8], (EXPERTS, D, FF), D ** -0.5, 0.125, ((0, 64), (2, 4)))
    expert_up = centred(key_list[9], (EXPERTS, D, FF), D ** -0.5, 0.125, ((0, 64), (2, 4)))
    expert_down = centred(key_list[10], (EXPERTS, FF, D), FF ** -0.5, 0.109375, ((0, 64), (1, 4)))
    return {"queries": queries, "key_value_pairs": key_value_pairs, "forget_gate_total": forget_gate_total, "residual_in": residual_in, "out_weight": out_weight, "norm_gain": norm_gain, "routes": routes, "route_weight": route_weight, "expert_gate": expert_gate, "expert_up": expert_up, "expert_down": expert_down}


NEG_FILL = -1e+30
NORM_EPS = 1e-06

def round_half(values):
    return lax.optimization_barrier(values.astype(jnp.bfloat16)).astype(jnp.float32)

def attention(queries, key_value_pairs, forget_gate_total):
    token_total = queries.shape[0]
    queries_per_group = QUERY_HEADS // KEY_VALUE_HEADS
    score_scale = HEAD_SIZE ** (-0.5)
    grouped_queries = queries.reshape(token_total, KEY_VALUE_HEADS, queries_per_group, HEAD_SIZE)
    key_value_head_list = key_value_pairs.reshape(token_total, KEY_VALUE_HEADS, 2 * HEAD_SIZE)
    key_rows = key_value_head_list[:, :, :HEAD_SIZE].astype(jnp.float32)
    value_rows = key_value_head_list[:, :, HEAD_SIZE:].astype(jnp.float32)
    gate_row_slice = forget_gate_total.reshape(token_total, KEY_VALUE_HEADS, queries_per_group)
    key_gate = jnp.transpose(gate_row_slice, (1, 2, 0))
    key_pos = jnp.arange(token_total, dtype=jnp.int32)
    query_count = math.gcd(token_total, 128)

    def query_block(block_index):
        first_row = block_index * query_count
        query_rows = lax.dynamic_slice_in_dim(grouped_queries, first_row, query_count, 0).astype(jnp.float32)
        query_gate = lax.dynamic_slice_in_dim(gate_row_slice, first_row, query_count, 0)
        scores = jnp.einsum('tkgd,skd->ktgs', query_rows, key_rows) * score_scale
        scores = scores + jnp.transpose(query_gate, (1, 0, 2))[..., None] - key_gate[:, None, :, :]
        query_pos = first_row + jnp.arange(query_count, dtype=jnp.int32)
        scores = jnp.where(key_pos[None, None, None, :] <= query_pos[None, :, None, None], scores, NEG_FILL)
        row_max = lax.optimization_barrier(jnp.max(scores, axis=3, keepdims=True))
        weights = jnp.exp(scores - row_max)
        totals = lax.optimization_barrier(jnp.sum(weights, axis=3))
        numer = jnp.einsum('ktgs,skd->ktgd', round_half(weights), value_rows)
        result = numer / totals[..., None]
        return jnp.transpose(result, (1, 0, 2, 3)).reshape(query_count, QUERY_HEADS * HEAD_SIZE).astype(jnp.bfloat16)
    blocks = lax.map(query_block, jnp.arange(token_total // query_count, dtype=jnp.int32))
    return blocks.reshape(token_total, QUERY_HEADS * HEAD_SIZE)

def apply_experts(normed, routes, route_weight, expert_gate, expert_up, expert_down):
    token_total = normed.shape[0]
    chosen = routes.reshape(-1)
    flat_weight = route_weight.reshape(-1)
    slot_count = chosen.shape[0]
    most_rows = N_SP * N_TP * CAPACITY
    unit_width = FF // N_TP

    def one_expert(totals, inputs):
        expert_index, w_gate, w_up, w_down = inputs
        picked = jnp.nonzero(chosen == expert_index, size=most_rows, fill_value=slot_count)[0].astype(jnp.int32)
        usable = picked < slot_count
        safe_slot = jnp.minimum(picked, slot_count - 1)
        token_rows = safe_slot // TOP
        input_rows = normed[token_rows]
        expert_sum = jnp.zeros((most_rows, D), jnp.float32)
        for column in range(N_TP):
            col_band = slice(column * unit_width, (column + 1) * unit_width)
            gate_value = jnp.dot(input_rows, w_gate[:, col_band], preferred_element_type=jnp.float32)
            up_value = jnp.dot(input_rows, w_up[:, col_band], preferred_element_type=jnp.float32)
            hidden_rows = (jax.nn.silu(gate_value) * up_value).astype(jnp.bfloat16)
            expert_sum = expert_sum + round_half(jnp.dot(hidden_rows, w_down[col_band, :], preferred_element_type=jnp.float32))
        weighted = jnp.where(usable, flat_weight[safe_slot], 0.0)[:, None] * round_half(expert_sum)
        return (totals.at[token_rows].add(weighted), None)
    start_totals = jnp.zeros((token_total, D), jnp.float32)
    totals, _ = lax.scan(one_expert, start_totals, (jnp.arange(EXPERTS, dtype=jnp.int32), expert_gate, expert_up, expert_down))
    return totals

def reference(queries, key_value_pairs, forget_gate_total, residual_in, out_weight, norm_gain, routes, route_weight, expert_gate, expert_up, expert_down):
    attended = attention(queries, key_value_pairs, forget_gate_total)
    head_width = QUERY_HEADS * HEAD_SIZE // N_TP
    mixed_rows = jnp.zeros((attended.shape[0], D), jnp.float32)
    for column in range(N_TP):
        col_band = slice(column * head_width, (column + 1) * head_width)
        mixed_rows = mixed_rows + round_half(jnp.dot(attended[:, col_band], out_weight[col_band, :], preferred_element_type=jnp.float32))
    hidden_state = residual_in.astype(jnp.float32) + mixed_rows
    normed = (hidden_state * lax.rsqrt(lax.optimization_barrier(jnp.mean(hidden_state * hidden_state, axis=1, keepdims=True)) + NORM_EPS) * norm_gain).astype(jnp.bfloat16)
    combined = apply_experts(normed, routes, route_weight, expert_gate, expert_up, expert_down)
    return (hidden_state + combined).astype(jnp.bfloat16)
```

```python
import functools
import math

import jax
import jax.numpy as jnp
from jax import lax
from jax.experimental import pallas as pl
from jax.experimental.pallas import tpu as pltpu
from jax.sharding import Mesh
from jax.sharding import PartitionSpec as P

SP = ("sp_0", "sp_1", "sp_2")
SP_TP = ("sp_0", "sp_1", "sp_2", "tp")
NORM_EPS = 1e-06
HEAD_SIZE = 64
NEG_FILL = -1e30
LOG2E = math.log2(math.e)
BLOCK = 256
HALF = 128
KEY_ROWS = 96
VALUE_ROWS = 64


def prep_body(kv_ref, gate_ref, out_ref):
    kv = kv_ref[...].astype(jnp.float32).T
    gate = gate_ref[...]
    high = gate.astype(jnp.bfloat16).astype(jnp.float32)
    rest = gate - high
    middle = rest.astype(jnp.bfloat16).astype(jnp.float32)
    low = rest - middle
    gates = jnp.concatenate([high, middle, low, jnp.zeros_like(gate)], axis=0)
    out_ref[...] = jnp.concatenate(
        [kv[:HEAD_SIZE], gates, kv[HEAD_SIZE:]], axis=0
    ).astype(jnp.bfloat16)


def prepare_keys(kv, gate_t):
    return pl.pallas_call(
        prep_body,
        out_shape=jax.ShapeDtypeStruct((KEY_ROWS + VALUE_ROWS, kv.shape[0]), jnp.bfloat16),
        name="prepare_keys",
    )(kv, gate_t)


def attend_body(index_ref, qa_ref, qb_ref, own_ref, other_ref, outa_ref, outb_ref, qt_ref, max_ref, acc_ref, *, blocks, heads):
    columns = heads * HALF
    step = 256
    own_index = index_ref[0]
    core = own_index % 2
    row = lax.broadcasted_iota(jnp.int32, (KEY_ROWS - HEAD_SIZE, columns), 0)
    head = lax.broadcasted_iota(jnp.int32, (KEY_ROWS - HEAD_SIZE, columns), 1) // HALF
    picks = jnp.where((row % heads == head) & (row < 3 * heads), -1.0, 0.0)
    for which, q_ref in ((0, qa_ref), (1, qb_ref)):
        qt = (q_ref[...].astype(jnp.float32) * (HEAD_SIZE**-0.5)).T
        qt = jnp.concatenate(
            [qt[h * HEAD_SIZE : (h + 1) * HEAD_SIZE] for h in range(heads)], axis=1
        )
        qt_ref[which] = jnp.concatenate([qt, picks], axis=0).astype(jnp.bfloat16)
    max_ref[...] = jnp.full(max_ref.shape, NEG_FILL, jnp.float32)
    acc_ref[...] = jnp.zeros(acc_ref.shape, jnp.float32)

    def attend(which, pair, first_row):
        tile = jnp.concatenate([own_ref[pair], other_ref[pair]], axis=1)
        keys = tile[:KEY_ROWS].astype(jnp.float32).T.astype(jnp.bfloat16)
        values = jnp.concatenate(
            [tile[KEY_ROWS:], jnp.ones((16, 2 * BLOCK), jnp.bfloat16)], axis=0
        )
        for at in range(0, columns, step):
            cols = slice(at, at + step)
            scores = jnp.dot(keys, qt_ref[which, :, cols], preferred_element_type=jnp.float32)
            if first_row is not None:
                k = lax.broadcasted_iota(jnp.int32, scores.shape, 0)
                t = lax.broadcasted_iota(jnp.int32, scores.shape, 1) % HALF
                start = jnp.where(k < BLOCK, core * BLOCK, (1 - core) * BLOCK - BLOCK)
                seen = pair * (2 * BLOCK) + start + k <= first_row + t
                scores = jnp.where(seen, scores, NEG_FILL)
            before = max_ref[which, :, cols]
            now = jnp.maximum(before, jnp.max(scores, axis=0, keepdims=True))
            weights = jnp.exp2((scores - now) * LOG2E)
            rescale = jnp.exp2((before - now) * LOG2E)
            max_ref[which, :, cols] = now
            acc_ref[which, :, cols] = acc_ref[which, :, cols] * rescale + jnp.dot(
                values, weights.astype(jnp.bfloat16), preferred_element_type=jnp.float32
            )

    for which, index, first in (
        (0, own_index, own_index * BLOCK),
        (1, blocks - 1 - own_index, (blocks - 1 - own_index) * BLOCK + HALF),
    ):
        last_pair = index // 2

        def full(pair, carry, which=which):
            attend(which, pair, None)
            return carry

        lax.fori_loop(0, last_pair, full, 0)
        attend(which, last_pair, first)

    for which, out_ref in ((0, outa_ref), (1, outb_ref)):
        acc = acc_ref[which]
        out = acc[:VALUE_ROWS] / acc[VALUE_ROWS : VALUE_ROWS + 1]
        out = jnp.concatenate([out[:, h * HALF : (h + 1) * HALF] for h in range(heads)], axis=0)
        out_ref[...] = out.T.astype(out_ref.dtype)


def attend_rows(index, qa, qb, own, other):
    heads = qa.shape[1] // HEAD_SIZE
    blocks = 2 * own.shape[0]
    columns = heads * HALF
    out = jax.ShapeDtypeStruct(qa.shape, jnp.bfloat16)
    vmem = pl.BlockSpec(memory_space=pltpu.VMEM)
    return pl.pallas_call(
        functools.partial(attend_body, blocks=blocks, heads=heads),
        in_specs=[pl.BlockSpec(memory_space=pltpu.SMEM)] + [vmem] * 4,
        out_specs=[vmem] * 2,
        out_shape=[out, out],
        scratch_shapes=[
            pltpu.VMEM((2, KEY_ROWS, columns), jnp.bfloat16),
            pltpu.VMEM((2, 1, columns), jnp.float32),
            pltpu.VMEM((2, VALUE_ROWS + 16, columns), jnp.float32),
        ],
        compiler_params=pltpu.CompilerParams(vmem_limit_bytes=48 * 1024 * 1024),
        name="attend_rows",
    )(index, qa, qb, own, other)


def cut_along(array, dim, devices):
    shape = array.shape
    tiles = array.reshape(*shape[:dim], devices, shape[dim] // devices, *shape[dim + 1 :])
    return jnp.moveaxis(tiles, dim, 0)


def sum_at_owner(array, axis, dim):
    devices = lax.axis_size(axis)
    tiles = lax.all_to_all(cut_along(array, dim, devices), axis, 0, 0, tiled=True)
    return jnp.sum(tiles.astype(jnp.float32), axis=0)


def slot_ranks(chosen, experts):
    onehot = (chosen[..., None] == jnp.arange(experts, dtype=jnp.int32)).astype(jnp.int32)
    earlier = jnp.cumsum(onehot, axis=-2) - onehot
    return jnp.sum(earlier * onehot, axis=-1)


def fill_slots(source_rows, target, slot_total, per_row):
    owner_slot = (
        jnp.zeros((slot_total,), jnp.int32)
        .at[target]
        .set(jnp.arange(1, target.shape[0] + 1, dtype=jnp.int32))
    )
    picked = source_rows[jnp.maximum(owner_slot - 1, 0) // per_row]
    return jnp.where((owner_slot > 0)[:, None], picked, jnp.zeros_like(picked))


def local(
    queries,
    key_value_pairs,
    forget_gate_total,
    residual_in,
    out_weight,
    norm_gain,
    routes,
    route_weight,
    expert_gate,
    expert_up,
    expert_down,
):
    seq_devices = lax.axis_size(SP)
    head_devices = lax.axis_size("tp")
    tok_rows = queries.shape[0]
    index = lax.axis_index(SP).astype(jnp.int32)
    mirror = [(i, seq_devices - 1 - i) for i in range(seq_devices)]
    mirrored_queries = lax.ppermute(queries[HALF:], SP, mirror)
    block = prepare_keys(key_value_pairs, forget_gate_total.T)
    own = lax.all_gather(lax.all_gather(block, "sp_1"), "sp_0")
    own = own.reshape(-1, *block.shape)
    other = lax.ppermute(own, "sp_2", [(0, 1), (1, 0)])
    first, second = attend_rows(index.reshape(1), queries[:HALF], mirrored_queries, own, other)
    second = lax.ppermute(second, SP, mirror)
    attended = jnp.concatenate([first, second], axis=0)
    own_rows = tok_rows // head_devices
    row_block = attended
    mixed_rows = sum_at_owner(
        jnp.dot(row_block, out_weight, preferred_element_type=jnp.float32).astype(jnp.bfloat16),
        "tp",
        0,
    )
    hidden_state = residual_in.astype(jnp.float32) + mixed_rows
    normed = (
        hidden_state
        * lax.rsqrt(jnp.mean(hidden_state * hidden_state, axis=1, keepdims=True) + NORM_EPS)
        * norm_gain
    ).astype(jnp.bfloat16)
    top_count = routes.shape[1]
    capacity = max(2, 3 * own_rows * top_count // (2 * seq_devices))
    model_width = normed.shape[1]
    chosen = routes.reshape(-1)
    target = chosen * capacity + slot_ranks(chosen, seq_devices)
    outgoing = fill_slots(normed, target, seq_devices * capacity, top_count).reshape(
        seq_devices, capacity, model_width
    )
    incoming = lax.all_to_all(outgoing, SP, split_axis=0, concat_axis=0, tiled=True)
    arrived = lax.all_gather(incoming, "tp", axis=0, tiled=True)
    flat_in = arrived.reshape(-1, model_width)
    gate_value = jnp.dot(flat_in, expert_gate[0], preferred_element_type=jnp.float32)
    up_value = jnp.dot(flat_in, expert_up[0], preferred_element_type=jnp.float32)
    hidden_rows = (
        (jax.nn.silu(gate_value) * up_value)
        .astype(jnp.bfloat16)
        .reshape(arrived.shape[0], capacity, -1)
    )
    row_block = hidden_rows
    summed = lax.psum_scatter(
        jnp.einsum(
            "rcf,fd->rcd", row_block, expert_down[0], preferred_element_type=jnp.float32
        ).astype(jnp.bfloat16),
        "tp",
        scatter_dimension=0,
        tiled=True,
    )
    returned = lax.all_to_all(summed, SP, split_axis=0, concat_axis=0, tiled=True)
    picked = returned.reshape(-1, model_width)[target].reshape(own_rows, top_count, model_width)
    combined = jnp.sum(picked.astype(jnp.float32) * route_weight[..., None], axis=1)
    return (hidden_state + combined).astype(jnp.bfloat16)


def solution(mesh):
    finer = Mesh(mesh.devices.reshape(8, 4, 2, mesh.shape["tp"]), ("sp_0", "sp_1", "sp_2", "tp"))
    in_specs = (
        P(SP, "tp"),
        P(SP, "tp"),
        P(SP, "tp"),
        P(SP_TP, None),
        P("tp", None),
        P(),
        P(SP_TP, None),
        P(SP_TP, None),
        P(SP, None, "tp"),
        P(SP, None, "tp"),
        P(SP, "tp", None),
    )
    out_specs = P(SP_TP, None)
    return jax.shard_map(local, mesh=finer, in_specs=in_specs, out_specs=out_specs, check_vma=False)
```

```python
import functools
import math

import jax
import jax.numpy as jnp
from jax import lax
from jax.experimental import pallas as pl
from jax.experimental.pallas import tpu as pltpu
from jax.sharding import Mesh
from jax.sharding import PartitionSpec as P

SP = ("sp_0", "sp_1", "sp_2")
SP_TP = ("sp_0", "sp_1", "sp_2", "tp")
NORM_EPS = 1e-06
HEAD_SIZE = 64
NEG_FILL = -1e30
LOG2E = math.log2(math.e)
BLOCK = 256
HALF = 128
KEY_ROWS = 96
VALUE_ROWS = 64


def prep_body(kv_ref, gate_ref, out_ref):
    kv = kv_ref[...].astype(jnp.float32).T
    gate = gate_ref[...]
    high = gate.astype(jnp.bfloat16).astype(jnp.float32)
    rest = gate - high
    middle = rest.astype(jnp.bfloat16).astype(jnp.float32)
    low = rest - middle
    gates = jnp.concatenate([high, middle, low, jnp.zeros_like(gate)], axis=0)
    out_ref[...] = jnp.concatenate(
        [kv[:HEAD_SIZE], gates, kv[HEAD_SIZE:]], axis=0
    ).astype(jnp.bfloat16)


def prepare_keys(kv, gate_t):
    return pl.pallas_call(
        prep_body,
        out_shape=jax.ShapeDtypeStruct((KEY_ROWS + VALUE_ROWS, kv.shape[0]), jnp.bfloat16),
        name="prepare_keys",
    )(kv, gate_t)


def attend_body(index_ref, qa_ref, qb_ref, own_ref, other_ref, outa_ref, outb_ref, qt_ref, max_ref, acc_ref, *, blocks, heads):
    columns = heads * HALF
    step = 256
    own_index = index_ref[0]
    core = own_index % 2
    row = lax.broadcasted_iota(jnp.int32, (KEY_ROWS - HEAD_SIZE, columns), 0)
    head = lax.broadcasted_iota(jnp.int32, (KEY_ROWS - HEAD_SIZE, columns), 1) // HALF
    picks = jnp.where((row % heads == head) & (row < 3 * heads), -1.0, 0.0)
    for which, q_ref in ((0, qa_ref), (1, qb_ref)):
        qt = (q_ref[...].astype(jnp.float32) * (HEAD_SIZE**-0.5)).T
        qt = jnp.concatenate(
            [qt[h * HEAD_SIZE : (h + 1) * HEAD_SIZE] for h in range(heads)], axis=1
        )
        qt_ref[which] = jnp.concatenate([qt, picks], axis=0).astype(jnp.bfloat16)
    max_ref[...] = jnp.full(max_ref.shape, NEG_FILL, jnp.float32)
    acc_ref[...] = jnp.zeros(acc_ref.shape, jnp.float32)

    def attend(which, pair, first_row):
        tile = jnp.concatenate([own_ref[pair], other_ref[pair]], axis=1)
        keys = tile[:KEY_ROWS].astype(jnp.float32).T.astype(jnp.bfloat16)
        values = jnp.concatenate(
            [tile[KEY_ROWS:], jnp.ones((16, 2 * BLOCK), jnp.bfloat16)], axis=0
        )
        for at in range(0, columns, step):
            cols = slice(at, at + step)
            scores = jnp.dot(keys, qt_ref[which, :, cols], preferred_element_type=jnp.float32)
            if first_row is not None:
                k = lax.broadcasted_iota(jnp.int32, scores.shape, 0)
                t = lax.broadcasted_iota(jnp.int32, scores.shape, 1) % HALF
                start = jnp.where(k < BLOCK, core * BLOCK, (1 - core) * BLOCK - BLOCK)
                seen = pair * (2 * BLOCK) + start + k <= first_row + t
                scores = jnp.where(seen, scores, NEG_FILL)
            before = max_ref[which, :, cols]
            now = jnp.maximum(before, jnp.max(scores, axis=0, keepdims=True))
            weights = jnp.exp2((scores - now) * LOG2E)
            rescale = jnp.exp2((before - now) * LOG2E)
            max_ref[which, :, cols] = now
            acc_ref[which, :, cols] = acc_ref[which, :, cols] * rescale + jnp.dot(
                values, weights.astype(jnp.bfloat16), preferred_element_type=jnp.float32
            )

    for which, index, first in (
        (0, own_index, own_index * BLOCK),
        (1, blocks - 1 - own_index, (blocks - 1 - own_index) * BLOCK + HALF),
    ):
        last_pair = index // 2

        def full(pair, carry, which=which):
            attend(which, pair, None)
            return carry

        lax.fori_loop(0, last_pair, full, 0)
        attend(which, last_pair, first)

    for which, out_ref in ((0, outa_ref), (1, outb_ref)):
        acc = acc_ref[which]
        out = acc[:VALUE_ROWS] / acc[VALUE_ROWS : VALUE_ROWS + 1]
        out = jnp.concatenate([out[:, h * HALF : (h + 1) * HALF] for h in range(heads)], axis=0)
        out_ref[...] = out.T.astype(out_ref.dtype)


def attend_rows(index, qa, qb, own, other):
    heads = qa.shape[1] // HEAD_SIZE
    blocks = 2 * own.shape[0]
    columns = heads * HALF
    out = jax.ShapeDtypeStruct(qa.shape, jnp.bfloat16)
    vmem = pl.BlockSpec(memory_space=pltpu.VMEM)
    return pl.pallas_call(
        functools.partial(attend_body, blocks=blocks, heads=heads),
        in_specs=[pl.BlockSpec(memory_space=pltpu.SMEM)] + [vmem] * 4,
        out_specs=[vmem] * 2,
        out_shape=[out, out],
        scratch_shapes=[
            pltpu.VMEM((2, KEY_ROWS, columns), jnp.bfloat16),
            pltpu.VMEM((2, 1, columns), jnp.float32),
            pltpu.VMEM((2, VALUE_ROWS + 16, columns), jnp.float32),
        ],
        compiler_params=pltpu.CompilerParams(vmem_limit_bytes=48 * 1024 * 1024),
        name="attend_rows",
    )(index, qa, qb, own, other)


def routing(routes_ref, experts):
    rows = routes_ref.shape[0]
    lanes = lax.broadcasted_iota(jnp.int32, (rows, experts), 1)
    first = (routes_ref[:, 0:1] == lanes).astype(jnp.float32)
    second = (routes_ref[:, 1:2] == lanes).astype(jnp.float32)
    named = first + second
    above = lax.broadcasted_iota(jnp.int32, (rows, rows), 1) < lax.broadcasted_iota(
        jnp.int32, (rows, rows), 0
    )
    earlier = jnp.dot(
        above.astype(jnp.bfloat16), named.astype(jnp.bfloat16), preferred_element_type=jnp.float32
    )
    return first, second, named, earlier


def dispatch_body(parts_ref, residual_ref, gain_ref, routes_ref, hidden_ref, slots_ref, *, capacity):
    mixed = jnp.sum(parts_ref[...].astype(jnp.float32), axis=0)
    hidden = residual_ref[...].astype(jnp.float32) + mixed
    hidden_ref[...] = hidden
    scale = lax.rsqrt(jnp.mean(hidden * hidden, axis=1, keepdims=True) + NORM_EPS)
    normed = (hidden * scale * gain_ref[...]).astype(jnp.bfloat16)
    experts = slots_ref.shape[1]
    _, _, named, earlier = routing(routes_ref, experts)
    for slot in range(capacity):
        chosen = jnp.where(earlier == slot, named, 0.0).T.astype(jnp.bfloat16)
        slots_ref[slot] = jnp.dot(chosen, normed, preferred_element_type=jnp.float32).astype(
            jnp.bfloat16
        )


def dispatch(parts, residual, gain, routes, experts, capacity):
    rows, width = residual.shape
    return pl.pallas_call(
        functools.partial(dispatch_body, capacity=capacity),
        out_shape=[
            jax.ShapeDtypeStruct((rows, width), jnp.float32),
            jax.ShapeDtypeStruct((capacity, experts, width), jnp.bfloat16),
        ],
        name="dispatch",
    )(parts, residual, gain.reshape(1, width), routes)


def combine_body(returned_ref, hidden_ref, routes_ref, weight_ref, out_ref):
    capacity, experts, _ = returned_ref.shape
    first, second, _, earlier = routing(routes_ref, experts)
    weight = first * weight_ref[:, 0:1] + second * weight_ref[:, 1:2]
    total = hidden_ref[...]
    for slot in range(capacity):
        rest = jnp.where(earlier == slot, weight, 0.0)
        rows = returned_ref[slot]
        for _ in range(3):
            piece = rest.astype(jnp.bfloat16)
            rest = rest - piece.astype(jnp.float32)
            total = total + jnp.dot(piece, rows, preferred_element_type=jnp.float32)
    out_ref[...] = total.astype(jnp.bfloat16)


def combine(returned, hidden, routes, route_weight):
    return pl.pallas_call(
        combine_body,
        out_shape=jax.ShapeDtypeStruct(hidden.shape, jnp.bfloat16),
        name="combine",
    )(returned, hidden, routes, route_weight)


def local(
    queries,
    key_value_pairs,
    forget_gate_total,
    residual_in,
    out_weight,
    norm_gain,
    routes,
    route_weight,
    expert_gate,
    expert_up,
    expert_down,
):
    seq_devices = lax.axis_size(SP)
    head_devices = lax.axis_size("tp")
    index = lax.axis_index(SP).astype(jnp.int32)
    mirror = [(i, seq_devices - 1 - i) for i in range(seq_devices)]
    up = [(i, (i + 1) % head_devices) for i in range(head_devices)]
    down = [(i, (i - 1) % head_devices) for i in range(head_devices)]

    def neighbours(array):
        return lax.ppermute(array, "tp", up), lax.ppermute(array, "tp", down)

    def opposite(before, after):
        half = before.shape[0] // 2
        return jnp.concatenate(
            [lax.ppermute(before[:half], "tp", up), lax.ppermute(after[half:], "tp", down)], axis=0
        )

    mirrored_queries = lax.ppermute(queries[HALF:], SP, mirror)
    block = prepare_keys(key_value_pairs, forget_gate_total.T)
    own = lax.all_gather(lax.all_gather(block, "sp_1"), "sp_0")
    own = own.reshape(-1, *block.shape)
    other = lax.ppermute(own, "sp_2", [(0, 1), (1, 0)])
    down_own = expert_down[0]
    down_before, down_after = neighbours(down_own)
    first, second = attend_rows(index.reshape(1), queries[:HALF], mirrored_queries, own, other)
    down_before, down_after, first, second = lax.optimization_barrier(
        (down_before, down_after, first, second)
    )
    down_across = opposite(down_before, down_after)
    second = lax.ppermute(second, SP, mirror)
    attended = jnp.concatenate([first, second], axis=0)
    partial = jnp.dot(attended, out_weight, preferred_element_type=jnp.float32).astype(jnp.bfloat16)
    parts = lax.all_to_all(
        partial.reshape(head_devices, -1, partial.shape[1]), "tp", 0, 0, tiled=True
    )
    own_rows, top_count = routes.shape
    capacity = max(2, 3 * own_rows * top_count // (2 * seq_devices))
    hidden_state, slots = dispatch(
        parts, residual_in, norm_gain, routes, seq_devices, capacity
    )
    width = slots.shape[2]
    incoming = lax.all_to_all(slots.transpose(1, 0, 2), SP, 0, 0, tiled=True)
    rows_own = incoming.transpose(1, 0, 2).reshape(-1, width)

    def units(rows):
        gate_value = jnp.dot(rows, expert_gate[0], preferred_element_type=jnp.float32)
        up_value = jnp.dot(rows, expert_up[0], preferred_element_type=jnp.float32)
        return (jax.nn.silu(gate_value) * up_value).astype(jnp.bfloat16)

    rows_before, rows_after = neighbours(rows_own)
    units_own = units(rows_own)
    rows_across = opposite(rows_before, rows_after)
    units_from_before = lax.ppermute(units(rows_after), "tp", up)
    units_from_after = lax.ppermute(units(rows_before), "tp", down)
    across = [(i, (i + 2) % head_devices) for i in range(head_devices)]
    units_from_across = lax.ppermute(units(rows_across), "tp", across)
    summed = jnp.dot(units_own, down_own, preferred_element_type=jnp.float32)
    for got, weight in (
        (units_from_before, down_before),
        (units_from_after, down_after),
        (units_from_across, down_across),
    ):
        summed = summed + jnp.dot(got, weight, preferred_element_type=jnp.float32)
    leaving = summed.astype(jnp.bfloat16).reshape(capacity, seq_devices, width).transpose(1, 0, 2)
    returned = lax.all_to_all(leaving, SP, 0, 0, tiled=True).transpose(1, 0, 2)
    return combine(returned, hidden_state, routes, route_weight)


def solution(mesh):
    finer = Mesh(mesh.devices.reshape(8, 4, 2, mesh.shape["tp"]), ("sp_0", "sp_1", "sp_2", "tp"))
    in_specs = (
        P(SP, "tp"),
        P(SP, "tp"),
        P(SP, "tp"),
        P(SP_TP, None),
        P("tp", None),
        P(),
        P(SP_TP, None),
        P(SP_TP, None),
        P(SP, None, "tp"),
        P(SP, None, "tp"),
        P(SP, "tp", None),
    )
    out_specs = P(SP_TP, None)
    return jax.shard_map(local, mesh=finer, in_specs=in_specs, out_specs=out_specs, check_vma=False)
```

```python
import functools
import math

import jax
import jax.numpy as jnp
from jax import lax
from jax.experimental import pallas as pl
from jax.experimental.pallas import tpu as pltpu
from jax.sharding import Mesh
from jax.sharding import PartitionSpec as P

SP = ("sp_0", "sp_1", "sp_2")
SP_TP = ("sp_0", "sp_1", "sp_2", "tp")
NORM_EPS = 1e-06
HEAD_SIZE = 64
NEG_FILL = -1e30
LOG2E = math.log2(math.e)
BLOCK = 256
HALF = 128
KEY_ROWS = 96
VALUE_ROWS = 64


SAFE_SCORE = 60.0


def bf16_pieces(values):
    high = values.astype(jnp.bfloat16).astype(jnp.float32)
    rest = values - high
    middle = rest.astype(jnp.bfloat16).astype(jnp.float32)
    return [high, middle, rest - middle]


def prep_body(kv_ref, gate_ref, out_ref):
    kv = kv_ref[...].astype(jnp.float32).T
    keys = kv[:HEAD_SIZE]
    square = jnp.sum(keys * keys, axis=0, keepdims=True) * 1.02
    ones = jnp.ones_like(square)
    zeros = jnp.zeros_like(square)
    out_ref[...] = jnp.concatenate(
        [keys, *bf16_pieces(gate_ref[...])] + [ones] * 3 + [square] + [zeros] * 4 + [kv[HEAD_SIZE:]],
        axis=0,
    ).astype(jnp.bfloat16)


def prepare_keys(kv, gate_t):
    return pl.pallas_call(
        prep_body,
        out_shape=jax.ShapeDtypeStruct((KEY_ROWS + VALUE_ROWS, kv.shape[0]), jnp.bfloat16),
        name="prepare_keys",
    )(kv, gate_t)


def attend_body(index_ref, qa_ref, qb_ref, own_ref, other_ref, out_ref, qt_ref, max_ref, acc_ref, *, blocks, heads):
    columns = heads * HALF
    step = 256
    own_index = index_ref[0]
    core = own_index % 2
    picked = 3 * heads
    row = lax.broadcasted_iota(jnp.int32, (picked, columns), 0)
    head = lax.broadcasted_iota(jnp.int32, (picked, columns), 1) // HALF
    picks = jnp.where(row % heads == head, -1.0, 0.0)
    largest_query = jnp.float32(0.0)
    mirror = blocks - 1 - own_index
    gates_at = slice(HEAD_SIZE, HEAD_SIZE + picked)
    gates_a = own_ref[own_index // 2, gates_at, :HALF].astype(jnp.float32)
    gates_b = other_ref[mirror // 2, gates_at, HALF:].astype(jnp.float32)
    for which, q_ref, gates in ((0, qa_ref, gates_a), (1, qb_ref, gates_b)):
        qt = (q_ref[...].astype(jnp.float32) * (HEAD_SIZE**-0.5)).T
        qt = jnp.concatenate(
            [qt[h * HEAD_SIZE : (h + 1) * HEAD_SIZE] for h in range(heads)], axis=1
        )
        largest_query = jnp.maximum(
            largest_query, jnp.max(jnp.sum(qt * qt, axis=0, keepdims=True))
        )
        pieces = [
            jnp.concatenate([gates[p + h : p + h + 1] for h in range(heads)], axis=1)
            for p in range(0, picked, heads)
        ]
        qt_ref[which] = jnp.concatenate(
            [qt, picks, *pieces, jnp.zeros((5, columns), jnp.float32)], axis=0
        ).astype(jnp.bfloat16)
    tail = slice(KEY_ROWS - 16, KEY_ROWS)
    squares = jnp.maximum(
        jnp.max(own_ref[:, tail].astype(jnp.float32), axis=0),
        jnp.max(other_ref[:, tail].astype(jnp.float32), axis=0),
    )
    largest_key = jnp.max(squares[11:12])
    bounded = largest_query * largest_key <= SAFE_SCORE**2
    acc_ref[...] = jnp.zeros(acc_ref.shape, jnp.float32)

    def operands(pair):
        tile = jnp.concatenate([own_ref[pair], other_ref[pair]], axis=1)
        keys = tile[:KEY_ROWS].astype(jnp.float32).T.astype(jnp.bfloat16)
        values = jnp.concatenate(
            [tile[KEY_ROWS:], jnp.ones((16, 2 * BLOCK), jnp.bfloat16)], axis=0
        )
        return keys, values

    def masked(scores, pair, first_row):
        k = lax.broadcasted_iota(jnp.int32, scores.shape, 0)
        t = lax.broadcasted_iota(jnp.int32, scores.shape, 1) % HALF
        start = jnp.where(k < BLOCK, core * BLOCK, (1 - core) * BLOCK - BLOCK)
        seen = pair * (2 * BLOCK) + start + k <= first_row + t
        return jnp.where(seen, scores, NEG_FILL)

    def plan(which):
        index = jnp.where(which == 0, own_index, blocks - 1 - own_index)
        return index // 2, index * BLOCK + which * HALF

    def plain(which, pair, first_row):
        keys, values = operands(pair)
        for at in range(0, columns, step):
            cols = slice(at, at + step)
            scores = jnp.dot(keys, qt_ref[which, :, cols], preferred_element_type=jnp.float32)
            if first_row is not None:
                scores = masked(scores, pair, first_row)
            weights = jnp.exp2(scores * LOG2E).astype(jnp.bfloat16)
            acc_ref[which, :, cols] += jnp.dot(values, weights, preferred_element_type=jnp.float32)

    def shifted(which, pair, first_row):
        keys, values = operands(pair)

        def chunk(c, carry):
            cols = pl.ds(pl.multiple_of(c * step, step), step)
            scores = jnp.dot(keys, qt_ref[which, :, cols], preferred_element_type=jnp.float32)
            scores = masked(scores, pair, first_row)
            before = max_ref[which, :, cols]
            now = jnp.maximum(before, jnp.max(scores, axis=0, keepdims=True))
            weights = jnp.exp2((scores - now) * LOG2E)
            rescale = jnp.exp2((before - now) * LOG2E)
            max_ref[which, :, cols] = now
            acc_ref[which, :, cols] = acc_ref[which, :, cols] * rescale + jnp.dot(
                values, weights.astype(jnp.bfloat16), preferred_element_type=jnp.float32
            )
            return carry

        lax.fori_loop(0, columns // step, chunk, 0)

    @pl.when(bounded)
    def _():
        def one(which, carry):
            last_pair, first_row = plan(which)

            def full(pair, inner):
                plain(which, pair, None)
                return inner

            lax.fori_loop(0, last_pair, full, 0)
            plain(which, last_pair, first_row)
            return carry

        lax.fori_loop(0, 2, one, 0)

    @pl.when(jnp.logical_not(bounded))
    def _():
        max_ref[...] = jnp.full(max_ref.shape, NEG_FILL, jnp.float32)

        def one(which, carry):
            last_pair, first_row = plan(which)

            def any_pair(pair, inner):
                shifted(which, pair, first_row)
                return inner

            lax.fori_loop(0, last_pair + 1, any_pair, 0)
            return carry

        lax.fori_loop(0, 2, one, 0)

    for which in range(2):
        acc = acc_ref[which]
        out = acc[:VALUE_ROWS] / acc[VALUE_ROWS : VALUE_ROWS + 1]
        out = jnp.concatenate([out[:, h * HALF : (h + 1) * HALF] for h in range(heads)], axis=0)
        out_ref[which] = out.T.astype(out_ref.dtype)


def attend_rows(index, qa, qb, own, other):
    heads = qa.shape[1] // HEAD_SIZE
    blocks = 2 * own.shape[0]
    columns = heads * HALF
    vmem = pl.BlockSpec(memory_space=pltpu.VMEM)
    return pl.pallas_call(
        functools.partial(attend_body, blocks=blocks, heads=heads),
        in_specs=[pl.BlockSpec(memory_space=pltpu.SMEM)] + [vmem] * 4,
        out_specs=vmem,
        out_shape=jax.ShapeDtypeStruct((2, *qa.shape), jnp.bfloat16),
        scratch_shapes=[
            pltpu.VMEM((2, KEY_ROWS, columns), jnp.bfloat16),
            pltpu.VMEM((2, 1, columns), jnp.float32),
            pltpu.VMEM((2, VALUE_ROWS + 16, columns), jnp.float32),
        ],
        compiler_params=pltpu.CompilerParams(vmem_limit_bytes=48 * 1024 * 1024),
        name="attend_rows",
    )(index, qa, qb, own, other)


def routing(routes_ref, experts):
    rows = routes_ref.shape[0]
    lanes = lax.broadcasted_iota(jnp.int32, (rows, experts), 1)
    first = (routes_ref[:, 0:1] == lanes).astype(jnp.float32)
    second = (routes_ref[:, 1:2] == lanes).astype(jnp.float32)
    named = first + second
    above = lax.broadcasted_iota(jnp.int32, (rows, rows), 1) < lax.broadcasted_iota(
        jnp.int32, (rows, rows), 0
    )
    earlier = jnp.dot(
        above.astype(jnp.bfloat16), named.astype(jnp.bfloat16), preferred_element_type=jnp.float32
    )
    return first, second, named, earlier


def dispatch_body(parts_ref, residual_ref, gain_ref, routes_ref, hidden_ref, slots_ref, *, capacity):
    mixed = jnp.sum(parts_ref[...].astype(jnp.float32), axis=0)
    hidden = residual_ref[...].astype(jnp.float32) + mixed
    hidden_ref[...] = hidden
    scale = lax.rsqrt(jnp.mean(hidden * hidden, axis=1, keepdims=True) + NORM_EPS)
    normed = (hidden * scale * gain_ref[...]).astype(jnp.bfloat16)
    experts = slots_ref.shape[1]
    _, _, named, earlier = routing(routes_ref, experts)
    for slot in range(capacity):
        chosen = jnp.where(earlier == slot, named, 0.0).T.astype(jnp.bfloat16)
        slots_ref[slot] = jnp.dot(chosen, normed, preferred_element_type=jnp.float32).astype(
            jnp.bfloat16
        )


def dispatch(parts, residual, gain, routes, experts, capacity):
    rows, width = residual.shape
    return pl.pallas_call(
        functools.partial(dispatch_body, capacity=capacity),
        out_shape=[
            jax.ShapeDtypeStruct((rows, width), jnp.float32),
            jax.ShapeDtypeStruct((capacity, experts, width), jnp.bfloat16),
        ],
        name="dispatch",
    )(parts, residual, gain.reshape(1, width), routes)


def combine_body(returned_ref, hidden_ref, routes_ref, weight_ref, out_ref):
    capacity, experts, _ = returned_ref.shape
    first, second, _, earlier = routing(routes_ref, experts)
    weight = first * weight_ref[:, 0:1] + second * weight_ref[:, 1:2]
    total = hidden_ref[...]
    for slot in range(capacity):
        rest = jnp.where(earlier == slot, weight, 0.0)
        rows = returned_ref[slot]
        for _ in range(3):
            piece = rest.astype(jnp.bfloat16)
            rest = rest - piece.astype(jnp.float32)
            total = total + jnp.dot(piece, rows, preferred_element_type=jnp.float32)
    out_ref[...] = total.astype(jnp.bfloat16)


def combine(returned, hidden, routes, route_weight):
    return pl.pallas_call(
        combine_body,
        out_shape=jax.ShapeDtypeStruct(hidden.shape, jnp.bfloat16),
        name="combine",
    )(returned, hidden, routes, route_weight)


def local(
    queries,
    key_value_pairs,
    forget_gate_total,
    residual_in,
    out_weight,
    norm_gain,
    routes,
    route_weight,
    expert_gate,
    expert_up,
    expert_down,
):
    seq_devices = lax.axis_size(SP)
    head_devices = lax.axis_size("tp")
    index = lax.axis_index(SP).astype(jnp.int32)
    mirror = [(i, seq_devices - 1 - i) for i in range(seq_devices)]
    up = [(i, (i + 1) % head_devices) for i in range(head_devices)]
    down = [(i, (i - 1) % head_devices) for i in range(head_devices)]

    def neighbours(array):
        return lax.ppermute(array, "tp", up), lax.ppermute(array, "tp", down)

    def opposite(before, after):
        half = before.shape[0] // 2
        return jnp.concatenate(
            [lax.ppermute(before[:half], "tp", up), lax.ppermute(after[half:], "tp", down)], axis=0
        )

    whole = [
        (i * head_devices + t, (i if 2 * t < head_devices else seq_devices - 1 - i) * head_devices + t)
        for i in range(seq_devices)
        for t in range(head_devices)
    ]
    flipped = 2 * lax.axis_index("tp") >= head_devices
    block = prepare_keys(key_value_pairs, forget_gate_total.T)
    mirrored_queries = lax.ppermute(queries[HALF:], SP, mirror)
    near = lax.all_gather(block, "sp_1")
    near, mirrored_queries = lax.optimization_barrier((near, mirrored_queries))
    own = lax.all_gather(near, "sp_0").reshape(-1, *block.shape)
    down_own = expert_down[0]
    down_before, down_after = neighbours(down_own)
    held_residual = lax.ppermute(residual_in, SP_TP, whole)
    held_routes = lax.ppermute(routes, SP_TP, whole)
    other = lax.ppermute(own, "sp_2", [(0, 1), (1, 0)])
    attended = attend_rows(index.reshape(1), queries[:HALF], mirrored_queries, own, other)
    down_before, down_after, attended = lax.optimization_barrier(
        (down_before, down_after, attended)
    )
    down_across = opposite(down_before, down_after)
    partial = jnp.dot(
        attended.reshape(-1, attended.shape[2]), out_weight, preferred_element_type=jnp.float32
    ).astype(jnp.bfloat16)
    parts = lax.all_to_all(
        partial.reshape(head_devices, -1, partial.shape[1]), "tp", 0, 0, tiled=True
    )
    own_rows, top_count = routes.shape
    capacity = max(2, 3 * own_rows * top_count // (2 * seq_devices))
    ranked_routes = jnp.where(flipped, seq_devices - 1 - held_routes, held_routes)
    held_hidden, slots = dispatch(
        parts, held_residual, norm_gain, ranked_routes, seq_devices, capacity
    )
    hidden_state = lax.ppermute(held_hidden, SP_TP, whole)
    width = slots.shape[2]
    ranks = [
        [(i if 2 * t < head_devices else seq_devices - 1 - i) * head_devices + t for i in range(seq_devices)]
        for t in range(head_devices)
    ]
    incoming = lax.all_to_all(
        slots.transpose(1, 0, 2), SP_TP, 0, 0, axis_index_groups=ranks, tiled=True
    )
    rows_own = incoming.transpose(1, 0, 2).reshape(-1, width)

    def units(rows):
        gate_value = jnp.dot(rows, expert_gate[0], preferred_element_type=jnp.float32)
        up_value = jnp.dot(rows, expert_up[0], preferred_element_type=jnp.float32)
        return (jax.nn.silu(gate_value) * up_value).astype(jnp.bfloat16)

    rows_before, rows_after = neighbours(rows_own)
    units_own = units(rows_own)
    rows_across = opposite(rows_before, rows_after)
    units_from_before = lax.ppermute(units(rows_after), "tp", up)
    units_from_after = lax.ppermute(units(rows_before), "tp", down)
    across = [(i, (i + 2) % head_devices) for i in range(head_devices)]
    units_from_across = lax.ppermute(units(rows_across), "tp", across)
    summed = jnp.dot(units_own, down_own, preferred_element_type=jnp.float32)
    for got, weight in (
        (units_from_before, down_before),
        (units_from_after, down_after),
        (units_from_across, down_across),
    ):
        summed = summed + jnp.dot(got, weight, preferred_element_type=jnp.float32)
    leaving = summed.astype(jnp.bfloat16).reshape(capacity, seq_devices, width).transpose(1, 0, 2)
    returned = lax.all_to_all(leaving, SP, 0, 0, tiled=True).transpose(1, 0, 2)
    return combine(returned, hidden_state, routes, route_weight)


def solution(mesh):
    finer = Mesh(mesh.devices.reshape(8, 4, 2, mesh.shape["tp"]), ("sp_0", "sp_1", "sp_2", "tp"))
    in_specs = (
        P(SP, "tp"),
        P(SP, "tp"),
        P(SP, "tp"),
        P(SP_TP, None),
        P("tp", None),
        P(),
        P(SP_TP, None),
        P(SP_TP, None),
        P(SP, None, "tp"),
        P(SP, None, "tp"),
        P(SP, "tp", None),
    )
    out_specs = P(SP_TP, None)
    return jax.shard_map(local, mesh=finer, in_specs=in_specs, out_specs=out_specs, check_vma=False)
```

```python
import functools
import math

import jax
import jax.numpy as jnp
from jax import lax
from jax.experimental import pallas as pl
from jax.experimental.pallas import tpu as pltpu
from jax.sharding import Mesh
from jax.sharding import PartitionSpec as P

SP = ("sp_0", "sp_1", "sp_2")
SP_TP = ("sp_0", "sp_1", "sp_2", "tp")
NORM_EPS = 1e-06
HEAD_SIZE = 64
NEG_FILL = -1e30
LOG2E = math.log2(math.e)
BLOCK = 256
HALF = 128
KEY_ROWS = 96
VALUE_ROWS = 64


SAFE_SCORE = 60.0
STEP = 512
PAIRS = 2


def bf16_pieces(values):
    high = values.astype(jnp.bfloat16).astype(jnp.float32)
    rest = values - high
    middle = rest.astype(jnp.bfloat16).astype(jnp.float32)
    return [high, middle, rest - middle]


def prep_body(kv_ref, gate_ref, out_ref):
    kv = kv_ref[...].astype(jnp.float32).T
    keys = kv[:HEAD_SIZE]
    square = jnp.sum(keys * keys, axis=0, keepdims=True) * 1.02
    ones = jnp.ones_like(square)
    zeros = jnp.zeros_like(square)
    out_ref[...] = jnp.concatenate(
        [keys, *bf16_pieces(gate_ref[...])] + [ones] * 3 + [square] + [zeros] * 4 + [kv[HEAD_SIZE:]],
        axis=0,
    ).astype(jnp.bfloat16)


def prepare_keys(kv, gate_t):
    return pl.pallas_call(
        prep_body,
        out_shape=jax.ShapeDtypeStruct((KEY_ROWS + VALUE_ROWS, kv.shape[0]), jnp.bfloat16),
        name="prepare_keys",
    )(kv, gate_t)


def attend_body(index_ref, qa_ref, qb_ref, own_ref, other_ref, out_ref, qt_ref, max_ref, acc_ref, *, blocks, heads):
    columns = heads * HALF
    step = STEP
    own_index = index_ref[0]
    core = own_index % 2
    picked = 3 * heads
    row = lax.broadcasted_iota(jnp.int32, (picked, columns), 0)
    head = lax.broadcasted_iota(jnp.int32, (picked, columns), 1) // HALF
    picks = jnp.where(row % heads == head, -1.0, 0.0)
    largest_query = jnp.float32(0.0)
    mirror = blocks - 1 - own_index
    gates_at = slice(HEAD_SIZE, HEAD_SIZE + picked)
    gates_a = own_ref[own_index // 2, gates_at, :HALF].astype(jnp.float32)
    gates_b = other_ref[mirror // 2, gates_at, HALF:].astype(jnp.float32)
    for which, q_ref, gates in ((0, qa_ref, gates_a), (1, qb_ref, gates_b)):
        qt = (q_ref[...].astype(jnp.float32) * (HEAD_SIZE**-0.5)).T
        qt = jnp.concatenate(
            [qt[h * HEAD_SIZE : (h + 1) * HEAD_SIZE] for h in range(heads)], axis=1
        )
        largest_query = jnp.maximum(
            largest_query, jnp.max(jnp.sum(qt * qt, axis=0, keepdims=True))
        )
        pieces = [
            jnp.concatenate([gates[p + h : p + h + 1] for h in range(heads)], axis=1)
            for p in range(0, picked, heads)
        ]
        qt_ref[which] = jnp.concatenate(
            [qt, picks, *pieces, jnp.zeros((5, columns), jnp.float32)], axis=0
        ).astype(jnp.bfloat16)
    tail = slice(KEY_ROWS - 16, KEY_ROWS)
    squares = jnp.maximum(
        jnp.max(own_ref[:, tail].astype(jnp.float32), axis=0),
        jnp.max(other_ref[:, tail].astype(jnp.float32), axis=0),
    )
    largest_key = jnp.max(squares[11:12])
    bounded = largest_query * largest_key <= SAFE_SCORE**2
    acc_ref[...] = jnp.zeros(acc_ref.shape, jnp.float32)

    def operands(pair, count=1):
        tile = jnp.concatenate(
            [r[pair + n] for n in range(count) for r in (own_ref, other_ref)], axis=1
        )
        keys = tile[:KEY_ROWS].astype(jnp.float32).T.astype(jnp.bfloat16)
        values = jnp.concatenate(
            [tile[KEY_ROWS:], jnp.ones((16, tile.shape[1]), jnp.bfloat16)], axis=0
        )
        return keys, values

    def masked(scores, pair, first_row):
        k = lax.broadcasted_iota(jnp.int32, scores.shape, 0)
        t = lax.broadcasted_iota(jnp.int32, scores.shape, 1) % HALF
        start = jnp.where(k < BLOCK, core * BLOCK, (1 - core) * BLOCK - BLOCK)
        seen = pair * (2 * BLOCK) + start + k <= first_row + t
        return jnp.where(seen, scores, NEG_FILL)

    def plan(which):
        index = jnp.where(which == 0, own_index, blocks - 1 - own_index)
        return index // 2, index * BLOCK + which * HALF

    def plain(which, pair, first_row, count=1):
        keys, values = operands(pair, count)
        for at in range(0, columns, step):
            cols = slice(at, at + step)
            scores = jnp.dot(keys, qt_ref[which, :, cols], preferred_element_type=jnp.float32)
            if first_row is not None:
                scores = masked(scores, pair, first_row)
            weights = jnp.exp2(scores * LOG2E).astype(jnp.bfloat16)
            acc_ref[which, :, cols] += jnp.dot(values, weights, preferred_element_type=jnp.float32)

    def shifted(which, pair, first_row):
        keys, values = operands(pair)

        def chunk(c, carry):
            cols = pl.ds(pl.multiple_of(c * step, step), step)
            scores = jnp.dot(keys, qt_ref[which, :, cols], preferred_element_type=jnp.float32)
            scores = masked(scores, pair, first_row)
            before = max_ref[which, :, cols]
            now = jnp.maximum(before, jnp.max(scores, axis=0, keepdims=True))
            weights = jnp.exp2((scores - now) * LOG2E)
            rescale = jnp.exp2((before - now) * LOG2E)
            max_ref[which, :, cols] = now
            acc_ref[which, :, cols] = acc_ref[which, :, cols] * rescale + jnp.dot(
                values, weights.astype(jnp.bfloat16), preferred_element_type=jnp.float32
            )
            return carry

        lax.fori_loop(0, columns // step, chunk, 0)

    @pl.when(bounded)
    def _():
        def one(which, carry):
            last_pair, first_row = plan(which)

            def full(pair, inner):
                plain(which, pair, None)
                return inner

            def many(group, inner):
                plain(which, group * PAIRS, None, PAIRS)
                return inner

            groups = last_pair // PAIRS
            if PAIRS > 1:
                lax.fori_loop(0, groups, many, 0)
                lax.fori_loop(groups * PAIRS, last_pair, full, 0)
            else:
                lax.fori_loop(0, last_pair, full, 0)
            plain(which, last_pair, first_row)
            return carry

        lax.fori_loop(0, 2, one, 0)

    @pl.when(jnp.logical_not(bounded))
    def _():
        max_ref[...] = jnp.full(max_ref.shape, NEG_FILL, jnp.float32)

        def one(which, carry):
            last_pair, first_row = plan(which)

            def any_pair(pair, inner):
                shifted(which, pair, first_row)
                return inner

            lax.fori_loop(0, last_pair + 1, any_pair, 0)
            return carry

        lax.fori_loop(0, 2, one, 0)

    for which in range(2):
        acc = acc_ref[which]
        out = acc[:VALUE_ROWS] / acc[VALUE_ROWS : VALUE_ROWS + 1]
        out = jnp.concatenate([out[:, h * HALF : (h + 1) * HALF] for h in range(heads)], axis=0)
        out_ref[which] = out.T.astype(out_ref.dtype)


def attend_rows(index, qa, qb, own, other):
    heads = qa.shape[1] // HEAD_SIZE
    blocks = 2 * own.shape[0]
    columns = heads * HALF
    vmem = pl.BlockSpec(memory_space=pltpu.VMEM)
    return pl.pallas_call(
        functools.partial(attend_body, blocks=blocks, heads=heads),
        in_specs=[pl.BlockSpec(memory_space=pltpu.SMEM)] + [vmem] * 4,
        out_specs=vmem,
        out_shape=jax.ShapeDtypeStruct((2, *qa.shape), jnp.bfloat16),
        scratch_shapes=[
            pltpu.VMEM((2, KEY_ROWS, columns), jnp.bfloat16),
            pltpu.VMEM((2, 1, columns), jnp.float32),
            pltpu.VMEM((2, VALUE_ROWS + 16, columns), jnp.float32),
        ],
        compiler_params=pltpu.CompilerParams(vmem_limit_bytes=48 * 1024 * 1024),
        name="attend_rows",
    )(index, qa, qb, own, other)


def routing(routes_ref, experts):
    rows = routes_ref.shape[0]
    lanes = lax.broadcasted_iota(jnp.int32, (rows, experts), 1)
    first = (routes_ref[:, 0:1] == lanes).astype(jnp.float32)
    second = (routes_ref[:, 1:2] == lanes).astype(jnp.float32)
    named = first + second
    above = lax.broadcasted_iota(jnp.int32, (rows, rows), 1) < lax.broadcasted_iota(
        jnp.int32, (rows, rows), 0
    )
    earlier = jnp.dot(
        above.astype(jnp.bfloat16), named.astype(jnp.bfloat16), preferred_element_type=jnp.float32
    )
    return first, second, named, earlier


def dispatch_body(parts_ref, residual_ref, gain_ref, routes_ref, hidden_ref, slots_ref, *, capacity):
    mixed = jnp.sum(parts_ref[...].astype(jnp.float32), axis=0)
    hidden = residual_ref[...].astype(jnp.float32) + mixed
    hidden_ref[...] = hidden
    scale = lax.rsqrt(jnp.mean(hidden * hidden, axis=1, keepdims=True) + NORM_EPS)
    normed = (hidden * scale * gain_ref[...]).astype(jnp.bfloat16)
    experts = slots_ref.shape[1]
    _, _, named, earlier = routing(routes_ref, experts)
    for slot in range(capacity):
        chosen = jnp.where(earlier == slot, named, 0.0).T.astype(jnp.bfloat16)
        slots_ref[slot] = jnp.dot(chosen, normed, preferred_element_type=jnp.float32).astype(
            jnp.bfloat16
        )


def dispatch(parts, residual, gain, routes, experts, capacity):
    rows, width = residual.shape
    return pl.pallas_call(
        functools.partial(dispatch_body, capacity=capacity),
        out_shape=[
            jax.ShapeDtypeStruct((rows, width), jnp.float32),
            jax.ShapeDtypeStruct((capacity, experts, width), jnp.bfloat16),
        ],
        name="dispatch",
    )(parts, residual, gain.reshape(1, width), routes)


def combine_body(returned_ref, hidden_ref, routes_ref, weight_ref, out_ref):
    capacity, experts, _ = returned_ref.shape
    first, second, _, earlier = routing(routes_ref, experts)
    weight = first * weight_ref[:, 0:1] + second * weight_ref[:, 1:2]
    total = hidden_ref[...]
    for slot in range(capacity):
        rest = jnp.where(earlier == slot, weight, 0.0)
        rows = returned_ref[slot]
        for _ in range(3):
            piece = rest.astype(jnp.bfloat16)
            rest = rest - piece.astype(jnp.float32)
            total = total + jnp.dot(piece, rows, preferred_element_type=jnp.float32)
    out_ref[...] = total.astype(jnp.bfloat16)


def combine(returned, hidden, routes, route_weight):
    return pl.pallas_call(
        combine_body,
        out_shape=jax.ShapeDtypeStruct(hidden.shape, jnp.bfloat16),
        name="combine",
    )(returned, hidden, routes, route_weight)


def local(
    queries,
    key_value_pairs,
    forget_gate_total,
    residual_in,
    out_weight,
    norm_gain,
    routes,
    route_weight,
    expert_gate,
    expert_up,
    expert_down,
):
    seq_devices = lax.axis_size(SP)
    head_devices = lax.axis_size("tp")
    index = lax.axis_index(SP).astype(jnp.int32)
    mirror = [(i, seq_devices - 1 - i) for i in range(seq_devices)]
    up = [(i, (i + 1) % head_devices) for i in range(head_devices)]
    down = [(i, (i - 1) % head_devices) for i in range(head_devices)]

    def neighbours(array):
        return lax.ppermute(array, "tp", up), lax.ppermute(array, "tp", down)

    def opposite(before, after):
        half = before.shape[0] // 2
        return jnp.concatenate(
            [lax.ppermute(before[:half], "tp", up), lax.ppermute(after[half:], "tp", down)], axis=0
        )

    whole = [
        (i * head_devices + t, (i if 2 * t < head_devices else seq_devices - 1 - i) * head_devices + t)
        for i in range(seq_devices)
        for t in range(head_devices)
    ]
    flipped = 2 * lax.axis_index("tp") >= head_devices
    block = prepare_keys(key_value_pairs, forget_gate_total.T)
    mirrored_queries = lax.ppermute(queries[HALF:], SP, mirror)
    near = lax.all_gather(block, "sp_1")
    near, mirrored_queries = lax.optimization_barrier((near, mirrored_queries))
    held_residual = lax.ppermute(residual_in, SP_TP, whole)
    held_routes = lax.ppermute(routes, SP_TP, whole)
    own = lax.all_gather(near, "sp_0").reshape(-1, *block.shape)
    own, held_residual, held_routes = lax.optimization_barrier((own, held_residual, held_routes))
    down_own = expert_down[0]
    down_before, down_after = neighbours(down_own)
    other = lax.ppermute(own, "sp_2", [(0, 1), (1, 0)])
    attended = attend_rows(index.reshape(1), queries[:HALF], mirrored_queries, own, other)
    down_before, down_after, attended = lax.optimization_barrier(
        (down_before, down_after, attended)
    )
    down_across = opposite(down_before, down_after)
    partial = jnp.dot(
        attended.reshape(-1, attended.shape[2]), out_weight, preferred_element_type=jnp.float32
    ).astype(jnp.bfloat16)
    parts = lax.all_to_all(
        partial.reshape(head_devices, -1, partial.shape[1]), "tp", 0, 0, tiled=True
    )
    own_rows, top_count = routes.shape
    capacity = max(2, 3 * own_rows * top_count // (2 * seq_devices))
    ranked_routes = jnp.where(flipped, seq_devices - 1 - held_routes, held_routes)
    held_hidden, slots = dispatch(
        parts, held_residual, norm_gain, ranked_routes, seq_devices, capacity
    )
    hidden_state = lax.ppermute(held_hidden, SP_TP, whole)
    width = slots.shape[2]
    ranks = [
        [(i if 2 * t < head_devices else seq_devices - 1 - i) * head_devices + t for i in range(seq_devices)]
        for t in range(head_devices)
    ]
    incoming = lax.all_to_all(
        slots.transpose(1, 0, 2), SP_TP, 0, 0, axis_index_groups=ranks, tiled=True
    )
    rows_own = incoming.transpose(1, 0, 2).reshape(-1, width)

    def units(rows):
        gate_value = jnp.dot(rows, expert_gate[0], preferred_element_type=jnp.float32)
        up_value = jnp.dot(rows, expert_up[0], preferred_element_type=jnp.float32)
        return (jax.nn.silu(gate_value) * up_value).astype(jnp.bfloat16)

    rows_before, rows_after = neighbours(rows_own)
    units_own = units(rows_own)
    rows_before, hidden_state = lax.optimization_barrier((rows_before, hidden_state))
    rows_across = opposite(rows_before, rows_after)
    units_from_before = lax.ppermute(units(rows_after), "tp", up)
    units_from_after = lax.ppermute(units(rows_before), "tp", down)
    across = [(i, (i + 2) % head_devices) for i in range(head_devices)]
    units_from_across = lax.ppermute(units(rows_across), "tp", across)
    summed = jnp.dot(units_own, down_own, preferred_element_type=jnp.float32)
    for got, weight in (
        (units_from_before, down_before),
        (units_from_after, down_after),
        (units_from_across, down_across),
    ):
        summed = summed + jnp.dot(got, weight, preferred_element_type=jnp.float32)
    leaving = summed.astype(jnp.bfloat16).reshape(capacity, seq_devices, width).transpose(1, 0, 2)
    returned = lax.all_to_all(leaving, SP, 0, 0, tiled=True).transpose(1, 0, 2)
    return combine(returned, hidden_state, routes, route_weight)


def solution(mesh):
    finer = Mesh(mesh.devices.reshape(8, 4, 2, mesh.shape["tp"]), ("sp_0", "sp_1", "sp_2", "tp"))
    in_specs = (
        P(SP, "tp"),
        P(SP, "tp"),
        P(SP, "tp"),
        P(SP_TP, None),
        P("tp", None),
        P(),
        P(SP_TP, None),
        P(SP_TP, None),
        P(SP, None, "tp"),
        P(SP, None, "tp"),
        P(SP, "tp", None),
    )
    out_specs = P(SP_TP, None)
    return jax.shard_map(local, mesh=finer, in_specs=in_specs, out_specs=out_specs, check_vma=False)
```

```python
import functools
import math

import jax
import jax.numpy as jnp
from jax import lax
from jax.experimental import pallas as pl
from jax.experimental.pallas import tpu as pltpu
from jax.sharding import Mesh
from jax.sharding import PartitionSpec as P

SP = ("sp_0", "sp_1", "sp_2")
SP_TP = ("sp_0", "sp_1", "sp_2", "tp")
NORM_EPS = 1e-06
HEAD_SIZE = 64
NEG_FILL = -1e30
LOG2E = math.log2(math.e)
BLOCK = 256
HALF = 128
KEY_ROWS = 96
VALUE_ROWS = 64


SAFE_SCORE = 60.0
STEP = 512
PAIRS = 2


def bf16_pieces(values):
    high = values.astype(jnp.bfloat16).astype(jnp.float32)
    rest = values - high
    middle = rest.astype(jnp.bfloat16).astype(jnp.float32)
    return [high, middle, rest - middle]


def prep_body(kv_ref, gate_ref, out_ref):
    kv = kv_ref[...].astype(jnp.float32).T
    keys = kv[:HEAD_SIZE]
    square = jnp.sum(keys * keys, axis=0, keepdims=True) * 1.02
    ones = jnp.ones_like(square)
    zeros = jnp.zeros_like(square)
    out_ref[...] = jnp.concatenate(
        [keys, *bf16_pieces(gate_ref[...])] + [ones] * 3 + [square] + [zeros] * 4 + [kv[HEAD_SIZE:]],
        axis=0,
    ).astype(jnp.bfloat16)


def prepare_keys(kv, gate_t):
    return pl.pallas_call(
        prep_body,
        out_shape=jax.ShapeDtypeStruct((KEY_ROWS + VALUE_ROWS, kv.shape[0]), jnp.bfloat16),
        name="prepare_keys",
    )(kv, gate_t)


def attend_body(index_ref, qa_ref, qb_ref, own_ref, other_ref, out_ref, qt_ref, max_ref, acc_ref, *, blocks, heads):
    columns = heads * HALF
    step = STEP
    own_index = index_ref[0]
    core = own_index % 2
    picked = 3 * heads
    row = lax.broadcasted_iota(jnp.int32, (picked, columns), 0)
    head = lax.broadcasted_iota(jnp.int32, (picked, columns), 1) // HALF
    picks = jnp.where(row % heads == head, -1.0, 0.0)
    largest_query = jnp.float32(0.0)
    mirror = blocks - 1 - own_index
    gates_at = slice(HEAD_SIZE, HEAD_SIZE + picked)
    gates_a = own_ref[own_index // 2, gates_at, :HALF].astype(jnp.float32)
    gates_b = other_ref[mirror // 2, gates_at, HALF:].astype(jnp.float32)
    for which, q_ref, gates in ((0, qa_ref, gates_a), (1, qb_ref, gates_b)):
        qt = (q_ref[...].astype(jnp.float32) * (HEAD_SIZE**-0.5)).T
        qt = jnp.concatenate(
            [qt[h * HEAD_SIZE : (h + 1) * HEAD_SIZE] for h in range(heads)], axis=1
        )
        largest_query = jnp.maximum(
            largest_query, jnp.max(jnp.sum(qt * qt, axis=0, keepdims=True))
        )
        pieces = [
            jnp.concatenate([gates[p + h : p + h + 1] for h in range(heads)], axis=1)
            for p in range(0, picked, heads)
        ]
        qt_ref[which] = jnp.concatenate(
            [qt, picks, *pieces, jnp.zeros((5, columns), jnp.float32)], axis=0
        ).astype(jnp.bfloat16)
    tail = slice(KEY_ROWS - 16, KEY_ROWS)
    squares = jnp.maximum(
        jnp.max(own_ref[:, tail].astype(jnp.float32), axis=0),
        jnp.max(other_ref[:, tail].astype(jnp.float32), axis=0),
    )
    largest_key = jnp.max(squares[11:12])
    bounded = largest_query * largest_key <= SAFE_SCORE**2
    acc_ref[...] = jnp.zeros(acc_ref.shape, jnp.float32)

    def operands(pair, count=1):
        tile = jnp.concatenate(
            [r[pair + n] for n in range(count) for r in (own_ref, other_ref)], axis=1
        )
        keys = tile[:KEY_ROWS].astype(jnp.float32).T.astype(jnp.bfloat16)
        values = jnp.concatenate(
            [tile[KEY_ROWS:], jnp.ones((16, tile.shape[1]), jnp.bfloat16)], axis=0
        )
        return keys, values

    def masked(scores, pair, first_row):
        k = lax.broadcasted_iota(jnp.int32, scores.shape, 0)
        t = lax.broadcasted_iota(jnp.int32, scores.shape, 1) % HALF
        start = jnp.where(k < BLOCK, core * BLOCK, (1 - core) * BLOCK - BLOCK)
        seen = pair * (2 * BLOCK) + start + k <= first_row + t
        return jnp.where(seen, scores, NEG_FILL)

    def plan(which):
        index = jnp.where(which == 0, own_index, blocks - 1 - own_index)
        return index // 2, index * BLOCK + which * HALF

    def plain(which, pair, first_row, count=1):
        keys, values = operands(pair, count)
        for at in range(0, columns, step):
            cols = slice(at, at + step)
            scores = jnp.dot(keys, qt_ref[which, :, cols], preferred_element_type=jnp.float32)
            if first_row is not None:
                scores = masked(scores, pair, first_row)
            weights = jnp.exp2(scores * LOG2E).astype(jnp.bfloat16)
            acc_ref[which, :, cols] += jnp.dot(values, weights, preferred_element_type=jnp.float32)

    def shifted(which, pair, first_row):
        keys, values = operands(pair)

        def chunk(c, carry):
            cols = pl.ds(pl.multiple_of(c * step, step), step)
            scores = jnp.dot(keys, qt_ref[which, :, cols], preferred_element_type=jnp.float32)
            scores = masked(scores, pair, first_row)
            before = max_ref[which, :, cols]
            now = jnp.maximum(before, jnp.max(scores, axis=0, keepdims=True))
            weights = jnp.exp2((scores - now) * LOG2E)
            rescale = jnp.exp2((before - now) * LOG2E)
            max_ref[which, :, cols] = now
            acc_ref[which, :, cols] = acc_ref[which, :, cols] * rescale + jnp.dot(
                values, weights.astype(jnp.bfloat16), preferred_element_type=jnp.float32
            )
            return carry

        lax.fori_loop(0, columns // step, chunk, 0)

    @pl.when(bounded)
    def _():
        def one(which, carry):
            last_pair, first_row = plan(which)

            def full(pair, inner):
                plain(which, pair, None)
                return inner

            def many(group, inner):
                plain(which, group * PAIRS, None, PAIRS)
                return inner

            groups = last_pair // PAIRS
            if PAIRS > 1:
                lax.fori_loop(0, groups, many, 0)
                lax.fori_loop(groups * PAIRS, last_pair, full, 0)
            else:
                lax.fori_loop(0, last_pair, full, 0)
            plain(which, last_pair, first_row)
            return carry

        lax.fori_loop(0, 2, one, 0)

    @pl.when(jnp.logical_not(bounded))
    def _():
        max_ref[...] = jnp.full(max_ref.shape, NEG_FILL, jnp.float32)

        def one(which, carry):
            last_pair, first_row = plan(which)

            def any_pair(pair, inner):
                shifted(which, pair, first_row)
                return inner

            lax.fori_loop(0, last_pair + 1, any_pair, 0)
            return carry

        lax.fori_loop(0, 2, one, 0)

    for which in range(2):
        acc = acc_ref[which]
        out = acc[:VALUE_ROWS] / acc[VALUE_ROWS : VALUE_ROWS + 1]
        out = jnp.concatenate([out[:, h * HALF : (h + 1) * HALF] for h in range(heads)], axis=0)
        out_ref[which] = out.T.astype(out_ref.dtype)


def attend_rows(index, qa, qb, own, other):
    heads = qa.shape[1] // HEAD_SIZE
    blocks = 2 * own.shape[0]
    columns = heads * HALF
    vmem = pl.BlockSpec(memory_space=pltpu.VMEM)
    return pl.pallas_call(
        functools.partial(attend_body, blocks=blocks, heads=heads),
        in_specs=[pl.BlockSpec(memory_space=pltpu.SMEM)] + [vmem] * 4,
        out_specs=vmem,
        out_shape=jax.ShapeDtypeStruct((2, *qa.shape), jnp.bfloat16),
        scratch_shapes=[
            pltpu.VMEM((2, KEY_ROWS, columns), jnp.bfloat16),
            pltpu.VMEM((2, 1, columns), jnp.float32),
            pltpu.VMEM((2, VALUE_ROWS + 16, columns), jnp.float32),
        ],
        compiler_params=pltpu.CompilerParams(vmem_limit_bytes=48 * 1024 * 1024),
        name="attend_rows",
    )(index, qa, qb, own, other)


def routing(routes_ref, experts):
    rows = routes_ref.shape[0]
    lanes = lax.broadcasted_iota(jnp.int32, (rows, experts), 1)
    first = (routes_ref[:, 0:1] == lanes).astype(jnp.float32)
    second = (routes_ref[:, 1:2] == lanes).astype(jnp.float32)
    named = first + second
    above = lax.broadcasted_iota(jnp.int32, (rows, rows), 1) < lax.broadcasted_iota(
        jnp.int32, (rows, rows), 0
    )
    earlier = jnp.dot(
        above.astype(jnp.bfloat16), named.astype(jnp.bfloat16), preferred_element_type=jnp.float32
    )
    return first, second, named, earlier


def spread_rows(tiles_ref, rows, slot, capacity):
    count, width = rows.shape
    per_row = width // 128
    for j in range(per_row):
        at = pl.ds(slot * per_row + j, count, stride=capacity * per_row)
        tiles_ref[at, :] = rows[:, j * 128 : (j + 1) * 128]


def joined_rows(tiles_ref, slot, capacity, count, width):
    per_row = width // 128
    return jnp.concatenate(
        [
            tiles_ref[pl.ds(slot * per_row + j, count, stride=capacity * per_row), :]
            for j in range(per_row)
        ],
        axis=1,
    )


def dispatch_body(parts_ref, residual_ref, gain_ref, routes_ref, hidden_ref, slots_ref, tiles_ref, *, capacity):
    mixed = jnp.sum(parts_ref[...].astype(jnp.float32), axis=0)
    hidden = residual_ref[...].astype(jnp.float32) + mixed
    hidden_ref[...] = hidden
    scale = lax.rsqrt(jnp.mean(hidden * hidden, axis=1, keepdims=True) + NORM_EPS)
    normed = (hidden * scale * gain_ref[...]).astype(jnp.bfloat16)
    experts = slots_ref.shape[0]
    _, _, named, earlier = routing(routes_ref, experts)
    for slot in range(capacity):
        chosen = jnp.where(earlier == slot, named, 0.0).T.astype(jnp.bfloat16)
        spread_rows(
            tiles_ref,
            jnp.dot(chosen, normed, preferred_element_type=jnp.float32),
            slot,
            capacity,
        )
    slots_ref[...] = tiles_ref[...].reshape(slots_ref.shape).astype(jnp.bfloat16)


def dispatch(parts, residual, gain, routes, experts, capacity):
    rows, width = residual.shape
    return pl.pallas_call(
        functools.partial(dispatch_body, capacity=capacity),
        out_shape=[
            jax.ShapeDtypeStruct((rows, width), jnp.float32),
            jax.ShapeDtypeStruct((experts, capacity * width // 128, 128), jnp.bfloat16),
        ],
        scratch_shapes=[pltpu.VMEM((experts * capacity * width // 128, 128), jnp.float32)],
        name="dispatch",
    )(parts, residual, gain.reshape(1, width), routes)


def arrange_body(arrived_ref, rows_ref, tiles_ref, *, capacity):
    count = arrived_ref.shape[0]
    tiles_ref[...] = arrived_ref[...].astype(jnp.float32).reshape(tiles_ref.shape)
    for slot in range(capacity):
        rows_ref[slot * count : (slot + 1) * count, :] = joined_rows(
            tiles_ref, slot, capacity, count, rows_ref.shape[1]
        ).astype(jnp.bfloat16)


def arrange(arrived, capacity):
    count, lines, lanes = arrived.shape
    return pl.pallas_call(
        functools.partial(arrange_body, capacity=capacity),
        out_shape=jax.ShapeDtypeStruct((capacity * count, lines * lanes // capacity), jnp.bfloat16),
        scratch_shapes=[pltpu.VMEM((count * lines, lanes), jnp.float32)],
        name="arrange",
    )(arrived)


def spread_body(rows_ref, leaving_ref, tiles_ref, *, capacity):
    count = leaving_ref.shape[0]
    for slot in range(capacity):
        spread_rows(tiles_ref, rows_ref[slot * count : (slot + 1) * count, :], slot, capacity)
    leaving_ref[...] = tiles_ref[...].reshape(leaving_ref.shape).astype(jnp.bfloat16)


def spread(rows, capacity):
    count, width = rows.shape[0] // capacity, rows.shape[1]
    lines = capacity * width // 128
    return pl.pallas_call(
        functools.partial(spread_body, capacity=capacity),
        out_shape=jax.ShapeDtypeStruct((count, lines, 128), jnp.bfloat16),
        scratch_shapes=[pltpu.VMEM((count * lines, 128), jnp.float32)],
        name="spread",
    )(rows)


def combine_body(returned_ref, hidden_ref, routes_ref, weight_ref, out_ref, tiles_ref, *, capacity):
    experts = returned_ref.shape[0]
    tiles_ref[...] = returned_ref[...].astype(jnp.float32).reshape(tiles_ref.shape)
    first, second, _, earlier = routing(routes_ref, experts)
    weight = first * weight_ref[:, 0:1] + second * weight_ref[:, 1:2]
    total = hidden_ref[...]
    for slot in range(capacity):
        rest = jnp.where(earlier == slot, weight, 0.0)
        rows = joined_rows(tiles_ref, slot, capacity, experts, out_ref.shape[1]).astype(jnp.bfloat16)
        for _ in range(3):
            piece = rest.astype(jnp.bfloat16)
            rest = rest - piece.astype(jnp.float32)
            total = total + jnp.dot(piece, rows, preferred_element_type=jnp.float32)
    out_ref[...] = total.astype(jnp.bfloat16)


def combine(returned, hidden, routes, route_weight, capacity):
    experts, lines, lanes = returned.shape
    return pl.pallas_call(
        functools.partial(combine_body, capacity=capacity),
        out_shape=jax.ShapeDtypeStruct(hidden.shape, jnp.bfloat16),
        scratch_shapes=[pltpu.VMEM((experts * lines, lanes), jnp.float32)],
        name="combine",
    )(returned, hidden, routes, route_weight)


def local(
    queries,
    key_value_pairs,
    forget_gate_total,
    residual_in,
    out_weight,
    norm_gain,
    routes,
    route_weight,
    expert_gate,
    expert_up,
    expert_down,
):
    seq_devices = lax.axis_size(SP)
    head_devices = lax.axis_size("tp")
    index = lax.axis_index(SP).astype(jnp.int32)
    mirror = [(i, seq_devices - 1 - i) for i in range(seq_devices)]
    up = [(i, (i + 1) % head_devices) for i in range(head_devices)]
    down = [(i, (i - 1) % head_devices) for i in range(head_devices)]

    def neighbours(array):
        return lax.ppermute(array, "tp", up), lax.ppermute(array, "tp", down)

    def opposite(before, after):
        half = before.shape[0] // 2
        return jnp.concatenate(
            [lax.ppermute(before[:half], "tp", up), lax.ppermute(after[half:], "tp", down)], axis=0
        )

    whole = [
        (i * head_devices + t, (i if 2 * t < head_devices else seq_devices - 1 - i) * head_devices + t)
        for i in range(seq_devices)
        for t in range(head_devices)
    ]
    flipped = 2 * lax.axis_index("tp") >= head_devices
    block = prepare_keys(key_value_pairs, forget_gate_total.T)
    mirrored_queries = lax.ppermute(queries[HALF:], SP, mirror)
    near = lax.all_gather(block, "sp_1")
    near, mirrored_queries = lax.optimization_barrier((near, mirrored_queries))
    held_residual = lax.ppermute(residual_in, SP_TP, whole)
    held_routes = lax.ppermute(routes, SP_TP, whole)
    own = lax.all_gather(near, "sp_0").reshape(-1, *block.shape)
    low, high = jnp.split(expert_down[0], 2)
    before_low, after_high = lax.ppermute(low, "tp", up), lax.ppermute(high, "tp", down)
    before_high, after_low = lax.ppermute(high, "tp", up), lax.ppermute(low, "tp", down)
    own, held_residual, held_routes, before_low, after_high = lax.optimization_barrier(
        (own, held_residual, held_routes, before_low, after_high)
    )
    other = lax.ppermute(own, "sp_2", [(0, 1), (1, 0)])
    attended = attend_rows(index.reshape(1), queries[:HALF], mirrored_queries, own, other)
    attended, before_high, after_low = lax.optimization_barrier((attended, before_high, after_low))
    across_low, across_high = lax.ppermute(before_low, "tp", up), lax.ppermute(after_high, "tp", down)
    partial = jnp.dot(
        attended.reshape(-1, attended.shape[2]), out_weight, preferred_element_type=jnp.float32
    ).astype(jnp.bfloat16)
    parts = lax.all_to_all(
        partial.reshape(head_devices, -1, partial.shape[1]), "tp", 0, 0, tiled=True
    )
    own_rows, top_count = routes.shape
    capacity = max(2, 3 * own_rows * top_count // (2 * seq_devices))
    ranked_routes = jnp.where(flipped, seq_devices - 1 - held_routes, held_routes)
    held_hidden, slots = dispatch(
        parts, held_residual, norm_gain, ranked_routes, seq_devices, capacity
    )
    slots, across_low, across_high = lax.optimization_barrier((slots, across_low, across_high))
    down_own = expert_down[0]
    down_before = jnp.concatenate([before_low, before_high])
    down_after = jnp.concatenate([after_low, after_high])
    down_across = jnp.concatenate([across_low, across_high])
    hidden_state = lax.ppermute(held_hidden, SP_TP, whole)
    ranks = [
        [(i if 2 * t < head_devices else seq_devices - 1 - i) * head_devices + t for i in range(seq_devices)]
        for t in range(head_devices)
    ]
    incoming = lax.all_to_all(
        slots, SP_TP, 0, 0, axis_index_groups=ranks, tiled=True
    )
    rows_own = arrange(incoming, capacity)

    def units(rows):
        gate_value = jnp.dot(rows, expert_gate[0], preferred_element_type=jnp.float32)
        up_value = jnp.dot(rows, expert_up[0], preferred_element_type=jnp.float32)
        return (jax.nn.silu(gate_value) * up_value).astype(jnp.bfloat16)

    rows_before, rows_after = neighbours(rows_own)
    units_own = units(rows_own)
    rows_across = opposite(rows_before, rows_after)
    rows_across, hidden_state = lax.optimization_barrier((rows_across, hidden_state))
    units_from_before = lax.ppermute(units(rows_after), "tp", up)
    units_from_after = lax.ppermute(units(rows_before), "tp", down)
    across = [(i, (i + 2) % head_devices) for i in range(head_devices)]
    units_from_across = lax.ppermute(units(rows_across), "tp", across)
    summed = jnp.dot(units_own, down_own, preferred_element_type=jnp.float32)
    for got, weight in (
        (units_from_before, down_before),
        (units_from_after, down_after),
        (units_from_across, down_across),
    ):
        summed = summed + jnp.dot(got, weight, preferred_element_type=jnp.float32)
    returned = lax.all_to_all(spread(summed, capacity), SP, 0, 0, tiled=True)
    return combine(returned, hidden_state, routes, route_weight, capacity)


def solution(mesh):
    finer = Mesh(mesh.devices.reshape(8, 4, 2, mesh.shape["tp"]), ("sp_0", "sp_1", "sp_2", "tp"))
    in_specs = (
        P(SP, "tp"),
        P(SP, "tp"),
        P(SP, "tp"),
        P(SP_TP, None),
        P("tp", None),
        P(),
        P(SP_TP, None),
        P(SP_TP, None),
        P(SP, None, "tp"),
        P(SP, None, "tp"),
        P(SP, "tp", None),
    )
    out_specs = P(SP_TP, None)
    return jax.shard_map(local, mesh=finer, in_specs=in_specs, out_specs=out_specs, check_vma=False)
```

```python
import functools
import math

import jax
import jax.numpy as jnp
from jax import lax
from jax.experimental import pallas as pl
from jax.experimental.pallas import tpu as pltpu
from jax.sharding import Mesh
from jax.sharding import PartitionSpec as P

SP = ("sp_0", "sp_1", "sp_2")
SP_TP = ("sp_0", "sp_1", "sp_2", "tp")
NORM_EPS = 1e-06
HEAD_SIZE = 64
NEG_FILL = -1e30
LOG2E = math.log2(math.e)
BLOCK = 256
HALF = 128
KEY_ROWS = 96
VALUE_ROWS = 64


SAFE_SCORE = 60.0
STEP = 512
PAIRS = 2


def bf16_pieces(values):
    high = values.astype(jnp.bfloat16).astype(jnp.float32)
    rest = values - high
    middle = rest.astype(jnp.bfloat16).astype(jnp.float32)
    return [high, middle, rest - middle]


def prep_body(kv_ref, gate_ref, out_ref):
    kv = kv_ref[...].astype(jnp.float32).T
    keys = kv[:HEAD_SIZE]
    square = jnp.sum(keys * keys, axis=0, keepdims=True) * 1.02
    ones = jnp.ones_like(square)
    zeros = jnp.zeros_like(square)
    out_ref[...] = jnp.concatenate(
        [keys, *bf16_pieces(gate_ref[...])] + [ones] * 3 + [square] + [zeros] * 4 + [kv[HEAD_SIZE:]],
        axis=0,
    ).astype(jnp.bfloat16)


def prepare_keys(kv, gate_t):
    return pl.pallas_call(
        prep_body,
        out_shape=jax.ShapeDtypeStruct((KEY_ROWS + VALUE_ROWS, kv.shape[0]), jnp.bfloat16),
        name="prepare_keys",
    )(kv, gate_t)


def attend_body(index_ref, qa_ref, qb_ref, own_ref, other_ref, out_ref, qt_ref, max_ref, acc_ref, *, blocks, heads):
    columns = heads * HALF
    step = STEP
    own_index = index_ref[0]
    core = own_index % 2
    picked = 3 * heads
    row = lax.broadcasted_iota(jnp.int32, (picked, columns), 0)
    head = lax.broadcasted_iota(jnp.int32, (picked, columns), 1) // HALF
    picks = jnp.where(row % heads == head, -1.0, 0.0)
    largest_query = jnp.float32(0.0)
    mirror = blocks - 1 - own_index
    gates_at = slice(HEAD_SIZE, HEAD_SIZE + picked)
    gates_a = own_ref[own_index // 2, gates_at, :HALF].astype(jnp.float32)
    gates_b = other_ref[mirror // 2, gates_at, HALF:].astype(jnp.float32)
    for which, q_ref, gates in ((0, qa_ref, gates_a), (1, qb_ref, gates_b)):
        qt = (q_ref[...].astype(jnp.float32) * (HEAD_SIZE**-0.5)).T
        qt = jnp.concatenate(
            [qt[h * HEAD_SIZE : (h + 1) * HEAD_SIZE] for h in range(heads)], axis=1
        )
        largest_query = jnp.maximum(
            largest_query, jnp.max(jnp.sum(qt * qt, axis=0, keepdims=True))
        )
        pieces = [
            jnp.concatenate([gates[p + h : p + h + 1] for h in range(heads)], axis=1)
            for p in range(0, picked, heads)
        ]
        qt_ref[which] = jnp.concatenate(
            [qt, picks, *pieces, jnp.zeros((5, columns), jnp.float32)], axis=0
        ).astype(jnp.bfloat16)
    tail = slice(KEY_ROWS - 16, KEY_ROWS)
    squares = jnp.maximum(
        jnp.max(own_ref[:, tail].astype(jnp.float32), axis=0),
        jnp.max(other_ref[:, tail].astype(jnp.float32), axis=0),
    )
    largest_key = jnp.max(squares[11:12])
    bounded = largest_query * largest_key <= SAFE_SCORE**2
    acc_ref[...] = jnp.zeros(acc_ref.shape, jnp.float32)

    def operands(pair, count=1):
        tile = jnp.concatenate(
            [r[pair + n] for n in range(count) for r in (own_ref, other_ref)], axis=1
        )
        keys = tile[:KEY_ROWS].astype(jnp.float32).T.astype(jnp.bfloat16)
        values = jnp.concatenate(
            [tile[KEY_ROWS:], jnp.ones((16, tile.shape[1]), jnp.bfloat16)], axis=0
        )
        return keys, values

    def masked(scores, pair, first_row):
        k = lax.broadcasted_iota(jnp.int32, scores.shape, 0)
        t = lax.broadcasted_iota(jnp.int32, scores.shape, 1) % HALF
        start = jnp.where(k < BLOCK, core * BLOCK, (1 - core) * BLOCK - BLOCK)
        seen = pair * (2 * BLOCK) + start + k <= first_row + t
        return jnp.where(seen, scores, NEG_FILL)

    def plan(which):
        index = jnp.where(which == 0, own_index, blocks - 1 - own_index)
        return index // 2, index * BLOCK + which * HALF

    def plain(which, pair, first_row, count=1):
        keys, values = operands(pair, count)
        for at in range(0, columns, step):
            cols = slice(at, at + step)
            scores = jnp.dot(keys, qt_ref[which, :, cols], preferred_element_type=jnp.float32)
            if first_row is not None:
                scores = masked(scores, pair, first_row)
            weights = jnp.exp2(scores * LOG2E).astype(jnp.bfloat16)
            acc_ref[which, :, cols] += jnp.dot(values, weights, preferred_element_type=jnp.float32)

    def shifted(which, pair, first_row):
        keys, values = operands(pair)

        def chunk(c, carry):
            cols = pl.ds(pl.multiple_of(c * step, step), step)
            scores = jnp.dot(keys, qt_ref[which, :, cols], preferred_element_type=jnp.float32)
            scores = masked(scores, pair, first_row)
            before = max_ref[which, :, cols]
            now = jnp.maximum(before, jnp.max(scores, axis=0, keepdims=True))
            weights = jnp.exp2((scores - now) * LOG2E)
            rescale = jnp.exp2((before - now) * LOG2E)
            max_ref[which, :, cols] = now
            acc_ref[which, :, cols] = acc_ref[which, :, cols] * rescale + jnp.dot(
                values, weights.astype(jnp.bfloat16), preferred_element_type=jnp.float32
            )
            return carry

        lax.fori_loop(0, columns // step, chunk, 0)

    @pl.when(bounded)
    def _():
        def one(which, carry):
            last_pair, first_row = plan(which)

            def full(pair, inner):
                plain(which, pair, None)
                return inner

            def many(group, inner):
                plain(which, group * PAIRS, None, PAIRS)
                return inner

            groups = last_pair // PAIRS
            if PAIRS > 1:
                lax.fori_loop(0, groups, many, 0)
                lax.fori_loop(groups * PAIRS, last_pair, full, 0)
            else:
                lax.fori_loop(0, last_pair, full, 0)
            plain(which, last_pair, first_row)
            return carry

        lax.fori_loop(0, 2, one, 0)

    @pl.when(jnp.logical_not(bounded))
    def _():
        max_ref[...] = jnp.full(max_ref.shape, NEG_FILL, jnp.float32)

        def one(which, carry):
            last_pair, first_row = plan(which)

            def any_pair(pair, inner):
                shifted(which, pair, first_row)
                return inner

            lax.fori_loop(0, last_pair + 1, any_pair, 0)
            return carry

        lax.fori_loop(0, 2, one, 0)

    for which in range(2):
        acc = acc_ref[which]
        out = acc[:VALUE_ROWS] / acc[VALUE_ROWS : VALUE_ROWS + 1]
        out = jnp.concatenate([out[:, h * HALF : (h + 1) * HALF] for h in range(heads)], axis=0)
        out_ref[which] = out.T.astype(out_ref.dtype)


def attend_rows(index, qa, qb, own, other):
    heads = qa.shape[1] // HEAD_SIZE
    blocks = 2 * own.shape[0]
    columns = heads * HALF
    vmem = pl.BlockSpec(memory_space=pltpu.VMEM)
    return pl.pallas_call(
        functools.partial(attend_body, blocks=blocks, heads=heads),
        in_specs=[pl.BlockSpec(memory_space=pltpu.SMEM)] + [vmem] * 4,
        out_specs=vmem,
        out_shape=jax.ShapeDtypeStruct((2, *qa.shape), jnp.bfloat16),
        scratch_shapes=[
            pltpu.VMEM((2, KEY_ROWS, columns), jnp.bfloat16),
            pltpu.VMEM((2, 1, columns), jnp.float32),
            pltpu.VMEM((2, VALUE_ROWS + 16, columns), jnp.float32),
        ],
        compiler_params=pltpu.CompilerParams(vmem_limit_bytes=48 * 1024 * 1024),
        name="attend_rows",
    )(index, qa, qb, own, other)


def routing(routes_ref, experts):
    rows = routes_ref.shape[0]
    lanes = lax.broadcasted_iota(jnp.int32, (rows, experts), 1)
    first = (routes_ref[:, 0:1] == lanes).astype(jnp.float32)
    second = (routes_ref[:, 1:2] == lanes).astype(jnp.float32)
    named = first + second
    above = lax.broadcasted_iota(jnp.int32, (rows, rows), 1) < lax.broadcasted_iota(
        jnp.int32, (rows, rows), 0
    )
    earlier = jnp.dot(
        above.astype(jnp.bfloat16), named.astype(jnp.bfloat16), preferred_element_type=jnp.float32
    )
    return first, second, named, earlier


def spread_rows(tiles_ref, rows, slot, capacity):
    count, width = rows.shape
    per_row = width // 128
    for j in range(per_row):
        at = pl.ds(slot * per_row + j, count, stride=capacity * per_row)
        tiles_ref[at, :] = rows[:, j * 128 : (j + 1) * 128]


def joined_rows(tiles_ref, slot, capacity, count, width):
    per_row = width // 128
    return jnp.concatenate(
        [
            tiles_ref[pl.ds(slot * per_row + j, count, stride=capacity * per_row), :]
            for j in range(per_row)
        ],
        axis=1,
    )


def dispatch_body(parts_ref, residual_ref, gain_ref, routes_ref, hidden_ref, slots_ref, tiles_ref, *, capacity):
    mixed = jnp.sum(parts_ref[...].astype(jnp.float32), axis=0)
    hidden = residual_ref[...].astype(jnp.float32) + mixed
    hidden_ref[...] = hidden
    scale = lax.rsqrt(jnp.mean(hidden * hidden, axis=1, keepdims=True) + NORM_EPS)
    normed = (hidden * scale * gain_ref[...]).astype(jnp.bfloat16)
    experts = slots_ref.shape[0]
    _, _, named, earlier = routing(routes_ref, experts)
    for slot in range(capacity):
        chosen = jnp.where(earlier == slot, named, 0.0).T.astype(jnp.bfloat16)
        spread_rows(
            tiles_ref,
            jnp.dot(chosen, normed, preferred_element_type=jnp.float32),
            slot,
            capacity,
        )
    slots_ref[...] = tiles_ref[...].reshape(slots_ref.shape).astype(jnp.bfloat16)


def dispatch(parts, residual, gain, routes, experts, capacity):
    rows, width = residual.shape
    return pl.pallas_call(
        functools.partial(dispatch_body, capacity=capacity),
        out_shape=[
            jax.ShapeDtypeStruct((rows, width), jnp.float32),
            jax.ShapeDtypeStruct((experts, capacity * width // 128, 128), jnp.bfloat16),
        ],
        scratch_shapes=[pltpu.VMEM((experts * capacity * width // 128, 128), jnp.float32)],
        name="dispatch",
    )(parts, residual, gain.reshape(1, width), routes)


def arrange_body(arrived_ref, rows_ref, tiles_ref, *, capacity):
    count = arrived_ref.shape[0]
    tiles_ref[...] = arrived_ref[...].astype(jnp.float32).reshape(tiles_ref.shape)
    for slot in range(capacity):
        rows_ref[slot * count : (slot + 1) * count, :] = joined_rows(
            tiles_ref, slot, capacity, count, rows_ref.shape[1]
        ).astype(jnp.bfloat16)


def arrange(arrived, capacity):
    count, lines, lanes = arrived.shape
    return pl.pallas_call(
        functools.partial(arrange_body, capacity=capacity),
        out_shape=jax.ShapeDtypeStruct((capacity * count, lines * lanes // capacity), jnp.bfloat16),
        scratch_shapes=[pltpu.VMEM((count * lines, lanes), jnp.float32)],
        name="arrange",
    )(arrived)


def spread_body(rows_ref, leaving_ref, tiles_ref, *, capacity):
    count = leaving_ref.shape[0]
    for slot in range(capacity):
        spread_rows(tiles_ref, rows_ref[slot * count : (slot + 1) * count, :], slot, capacity)
    leaving_ref[...] = tiles_ref[...].reshape(leaving_ref.shape).astype(jnp.bfloat16)


def spread(rows, capacity):
    count, width = rows.shape[0] // capacity, rows.shape[1]
    lines = capacity * width // 128
    return pl.pallas_call(
        functools.partial(spread_body, capacity=capacity),
        out_shape=jax.ShapeDtypeStruct((count, lines, 128), jnp.bfloat16),
        scratch_shapes=[pltpu.VMEM((count * lines, 128), jnp.float32)],
        name="spread",
    )(rows)


def combine_body(returned_ref, hidden_ref, routes_ref, weight_ref, out_ref, tiles_ref, *, capacity):
    experts = returned_ref.shape[0]
    tiles_ref[...] = returned_ref[...].astype(jnp.float32).reshape(tiles_ref.shape)
    first, second, _, earlier = routing(routes_ref, experts)
    weight = first * weight_ref[:, 0:1] + second * weight_ref[:, 1:2]
    total = hidden_ref[...]
    for slot in range(capacity):
        rest = jnp.where(earlier == slot, weight, 0.0)
        rows = joined_rows(tiles_ref, slot, capacity, experts, out_ref.shape[1]).astype(jnp.bfloat16)
        for _ in range(3):
            piece = rest.astype(jnp.bfloat16)
            rest = rest - piece.astype(jnp.float32)
            total = total + jnp.dot(piece, rows, preferred_element_type=jnp.float32)
    out_ref[...] = total.astype(jnp.bfloat16)


def combine(returned, hidden, routes, route_weight, capacity):
    experts, lines, lanes = returned.shape
    return pl.pallas_call(
        functools.partial(combine_body, capacity=capacity),
        out_shape=jax.ShapeDtypeStruct(hidden.shape, jnp.bfloat16),
        scratch_shapes=[pltpu.VMEM((experts * lines, lanes), jnp.float32)],
        name="combine",
    )(returned, hidden, routes, route_weight)


def layer(
    queries,
    key_value_pairs,
    forget_gate_total,
    residual_in,
    out_weight,
    norm_gain,
    routes,
    route_weight,
    expert_gate,
    expert_up,
    expert_down,
):
    seq_devices = lax.axis_size(SP)
    head_devices = lax.axis_size("tp")
    index = lax.axis_index(SP).astype(jnp.int32)
    mirror = [(i, seq_devices - 1 - i) for i in range(seq_devices)]
    up = [(i, (i + 1) % head_devices) for i in range(head_devices)]
    down = [(i, (i - 1) % head_devices) for i in range(head_devices)]

    def neighbours(array):
        return lax.ppermute(array, "tp", up), lax.ppermute(array, "tp", down)

    def opposite(before, after):
        half = before.shape[0] // 2
        return jnp.concatenate(
            [lax.ppermute(before[:half], "tp", up), lax.ppermute(after[half:], "tp", down)], axis=0
        )

    whole = [
        (i * head_devices + t, (i if 2 * t < head_devices else seq_devices - 1 - i) * head_devices + t)
        for i in range(seq_devices)
        for t in range(head_devices)
    ]
    flipped = 2 * lax.axis_index("tp") >= head_devices
    block = prepare_keys(key_value_pairs, forget_gate_total.T)
    mirrored_queries = lax.ppermute(queries[HALF:], SP, mirror)
    down_own = expert_down[0]
    down_before = lax.ppermute(down_own, "tp", up)
    down_after = lax.ppermute(down_own, "tp", down)
    near = lax.all_gather(block, "sp_1")
    near, mirrored_queries = lax.optimization_barrier((near, mirrored_queries))
    held_residual = lax.ppermute(residual_in, SP_TP, whole)
    held_routes = lax.ppermute(routes, SP_TP, whole)
    own = lax.all_gather(near, "sp_0").reshape(-1, *block.shape)
    own, held_residual, held_routes = lax.optimization_barrier((own, held_residual, held_routes))
    other = lax.ppermute(own, "sp_2", [(0, 1), (1, 0)])
    attended = attend_rows(index.reshape(1), queries[:HALF], mirrored_queries, own, other)
    down_before, down_after, attended = lax.optimization_barrier(
        (down_before, down_after, attended)
    )
    half = down_own.shape[0] // 2
    across_low = lax.ppermute(down_before[:half], "tp", up)
    across_high = lax.ppermute(down_after[half:], "tp", down)
    partial = jnp.dot(
        attended.reshape(-1, attended.shape[2]), out_weight, preferred_element_type=jnp.float32
    ).astype(jnp.bfloat16)
    parts = lax.all_to_all(
        partial.reshape(head_devices, -1, partial.shape[1]), "tp", 0, 0, tiled=True
    )
    own_rows, top_count = routes.shape
    capacity = max(2, 3 * own_rows * top_count // (2 * seq_devices))
    ranked_routes = jnp.where(flipped, seq_devices - 1 - held_routes, held_routes)
    held_hidden, slots = dispatch(
        parts, held_residual, norm_gain, ranked_routes, seq_devices, capacity
    )
    down_across = jnp.concatenate([across_low, across_high])
    hidden_state = lax.ppermute(held_hidden, SP_TP, whole)
    ranks = [
        [(i if 2 * t < head_devices else seq_devices - 1 - i) * head_devices + t for i in range(seq_devices)]
        for t in range(head_devices)
    ]
    incoming = lax.all_to_all(
        slots, SP_TP, 0, 0, axis_index_groups=ranks, tiled=True
    )
    rows_own = arrange(incoming, capacity)

    def units(rows):
        gate_value = jnp.dot(rows, expert_gate[0], preferred_element_type=jnp.float32)
        up_value = jnp.dot(rows, expert_up[0], preferred_element_type=jnp.float32)
        return (jax.nn.silu(gate_value) * up_value).astype(jnp.bfloat16)

    rows_before, rows_after = neighbours(rows_own)
    units_own = units(rows_own)
    rows_across = opposite(rows_before, rows_after)
    rows_across, hidden_state = lax.optimization_barrier((rows_across, hidden_state))
    units_from_before = lax.ppermute(units(rows_after), "tp", up)
    units_from_after = lax.ppermute(units(rows_before), "tp", down)
    across = [(i, (i + 2) % head_devices) for i in range(head_devices)]
    units_from_across = lax.ppermute(units(rows_across), "tp", across)
    summed = jnp.dot(units_own, down_own, preferred_element_type=jnp.float32)
    for got, weight in (
        (units_from_before, down_before),
        (units_from_after, down_after),
        (units_from_across, down_across),
    ):
        summed = summed + jnp.dot(got, weight, preferred_element_type=jnp.float32)
    returned = lax.all_to_all(spread(summed, capacity), SP, 0, 0, tiled=True)
    return combine(returned, hidden_state, routes, route_weight, capacity)


def solution(mesh):
    finer = Mesh(mesh.devices.reshape(8, 4, 2, mesh.shape["tp"]), ("sp_0", "sp_1", "sp_2", "tp"))
    in_specs = (
        P(SP, "tp"),
        P(SP, "tp"),
        P(SP, "tp"),
        P(SP_TP, None),
        P("tp", None),
        P(),
        P(SP_TP, None),
        P(SP_TP, None),
        P(SP, None, "tp"),
        P(SP, None, "tp"),
        P(SP, "tp", None),
    )
    out_specs = P(SP_TP, None)
    return jax.shard_map(layer, mesh=finer, in_specs=in_specs, out_specs=out_specs, check_vma=False)
```

```python
import functools
import math

import jax
import jax.numpy as jnp
from jax import lax
from jax.experimental import pallas as pl
from jax.experimental.pallas import tpu as pltpu
from jax.sharding import Mesh
from jax.sharding import PartitionSpec as P

SP = ("sp_0", "sp_1", "sp_2")
SP_TP = ("sp_0", "sp_1", "sp_2", "tp")
NORM_EPS = 1e-06
HEAD_SIZE = 64
NEG_FILL = -1e30
LOG2E = math.log2(math.e)
BLOCK = 256
HALF = 128
KEY_ROWS = 96
VALUE_ROWS = 64


SAFE_SCORE = 60.0
STEP = 512
PAIRS = 2


def bf16_pieces(values):
    high = values.astype(jnp.bfloat16).astype(jnp.float32)
    rest = values - high
    middle = rest.astype(jnp.bfloat16).astype(jnp.float32)
    return [high, middle, rest - middle]


def prep_body(kv_ref, gate_ref, out_ref):
    kv = kv_ref[...].astype(jnp.float32).T
    keys = kv[:HEAD_SIZE]
    square = jnp.sum(keys * keys, axis=0, keepdims=True) * 1.02
    ones = jnp.ones_like(square)
    zeros = jnp.zeros_like(square)
    out_ref[...] = jnp.concatenate(
        [keys, *bf16_pieces(gate_ref[...])] + [ones] * 3 + [square] + [zeros] * 4 + [kv[HEAD_SIZE:]],
        axis=0,
    ).astype(jnp.bfloat16)


def prepare_keys(kv, gate_t):
    return pl.pallas_call(
        prep_body,
        out_shape=jax.ShapeDtypeStruct((KEY_ROWS + VALUE_ROWS, kv.shape[0]), jnp.bfloat16),
        name="prepare_keys",
    )(kv, gate_t)


def attend_body(index_ref, qa_ref, qb_ref, own_ref, other_ref, out_ref, qt_ref, max_ref, acc_ref, *, blocks, heads):
    columns = heads * HALF
    step = STEP
    own_index = index_ref[0]
    core = own_index % 2
    picked = 3 * heads
    row = lax.broadcasted_iota(jnp.int32, (picked, columns), 0)
    head = lax.broadcasted_iota(jnp.int32, (picked, columns), 1) // HALF
    picks = jnp.where(row % heads == head, -1.0, 0.0)
    largest_query = jnp.float32(0.0)
    mirror = blocks - 1 - own_index
    gates_at = slice(HEAD_SIZE, HEAD_SIZE + picked)
    gates_a = own_ref[own_index // 2, gates_at, :HALF].astype(jnp.float32)
    gates_b = other_ref[mirror // 2, gates_at, HALF:].astype(jnp.float32)
    for which, q_ref, gates in ((0, qa_ref, gates_a), (1, qb_ref, gates_b)):
        qt = (q_ref[...].astype(jnp.float32) * (HEAD_SIZE**-0.5)).T
        qt = jnp.concatenate(
            [qt[h * HEAD_SIZE : (h + 1) * HEAD_SIZE] for h in range(heads)], axis=1
        )
        largest_query = jnp.maximum(
            largest_query, jnp.max(jnp.sum(qt * qt, axis=0, keepdims=True))
        )
        pieces = [
            jnp.concatenate([gates[p + h : p + h + 1] for h in range(heads)], axis=1)
            for p in range(0, picked, heads)
        ]
        qt_ref[which] = jnp.concatenate(
            [qt, picks, *pieces, jnp.zeros((5, columns), jnp.float32)], axis=0
        ).astype(jnp.bfloat16)
    tail = slice(KEY_ROWS - 16, KEY_ROWS)
    squares = jnp.maximum(
        jnp.max(own_ref[:, tail].astype(jnp.float32), axis=0),
        jnp.max(other_ref[:, tail].astype(jnp.float32), axis=0),
    )
    largest_key = jnp.max(squares[11:12])
    bounded = largest_query * largest_key <= SAFE_SCORE**2
    acc_ref[...] = jnp.zeros(acc_ref.shape, jnp.float32)

    def operands(pair, count=1):
        tile = jnp.concatenate(
            [r[pair + n] for n in range(count) for r in (own_ref, other_ref)], axis=1
        )
        keys = tile[:KEY_ROWS].astype(jnp.float32).T.astype(jnp.bfloat16)
        values = jnp.concatenate(
            [tile[KEY_ROWS:], jnp.ones((16, tile.shape[1]), jnp.bfloat16)], axis=0
        )
        return keys, values

    def masked(scores, pair, first_row):
        k = lax.broadcasted_iota(jnp.int32, scores.shape, 0)
        t = lax.broadcasted_iota(jnp.int32, scores.shape, 1) % HALF
        start = jnp.where(k < BLOCK, core * BLOCK, (1 - core) * BLOCK - BLOCK)
        seen = pair * (2 * BLOCK) + start + k <= first_row + t
        return jnp.where(seen, scores, NEG_FILL)

    def plan(which):
        index = jnp.where(which == 0, own_index, blocks - 1 - own_index)
        return index // 2, index * BLOCK + which * HALF

    def plain(which, pair, first_row, count=1):
        keys, values = operands(pair, count)
        for at in range(0, columns, step):
            cols = slice(at, at + step)
            scores = jnp.dot(keys, qt_ref[which, :, cols], preferred_element_type=jnp.float32)
            if first_row is not None:
                scores = masked(scores, pair, first_row)
            weights = jnp.exp2(scores * LOG2E).astype(jnp.bfloat16)
            acc_ref[which, :, cols] += jnp.dot(values, weights, preferred_element_type=jnp.float32)

    def shifted(which, pair, first_row):
        keys, values = operands(pair)

        def chunk(c, carry):
            cols = pl.ds(pl.multiple_of(c * step, step), step)
            scores = jnp.dot(keys, qt_ref[which, :, cols], preferred_element_type=jnp.float32)
            scores = masked(scores, pair, first_row)
            before = max_ref[which, :, cols]
            now = jnp.maximum(before, jnp.max(scores, axis=0, keepdims=True))
            weights = jnp.exp2((scores - now) * LOG2E)
            rescale = jnp.exp2((before - now) * LOG2E)
            max_ref[which, :, cols] = now
            acc_ref[which, :, cols] = acc_ref[which, :, cols] * rescale + jnp.dot(
                values, weights.astype(jnp.bfloat16), preferred_element_type=jnp.float32
            )
            return carry

        lax.fori_loop(0, columns // step, chunk, 0)

    @pl.when(bounded)
    def _():
        def one(which, carry):
            last_pair, first_row = plan(which)

            def full(pair, inner):
                plain(which, pair, None)
                return inner

            def many(group, inner):
                plain(which, group * PAIRS, None, PAIRS)
                return inner

            groups = last_pair // PAIRS
            if PAIRS > 1:
                lax.fori_loop(0, groups, many, 0)
                lax.fori_loop(groups * PAIRS, last_pair, full, 0)
            else:
                lax.fori_loop(0, last_pair, full, 0)
            plain(which, last_pair, first_row)
            return carry

        lax.fori_loop(0, 2, one, 0)

    @pl.when(jnp.logical_not(bounded))
    def _():
        max_ref[...] = jnp.full(max_ref.shape, NEG_FILL, jnp.float32)

        def one(which, carry):
            last_pair, first_row = plan(which)

            def any_pair(pair, inner):
                shifted(which, pair, first_row)
                return inner

            lax.fori_loop(0, last_pair + 1, any_pair, 0)
            return carry

        lax.fori_loop(0, 2, one, 0)

    for which in range(2):
        acc = acc_ref[which]
        out = acc[:VALUE_ROWS] / acc[VALUE_ROWS : VALUE_ROWS + 1]
        out = jnp.concatenate([out[:, h * HALF : (h + 1) * HALF] for h in range(heads)], axis=0)
        out_ref[which] = out.T.astype(out_ref.dtype)


def attend_rows(index, qa, qb, own, other):
    heads = qa.shape[1] // HEAD_SIZE
    blocks = 2 * own.shape[0]
    columns = heads * HALF
    vmem = pl.BlockSpec(memory_space=pltpu.VMEM)
    return pl.pallas_call(
        functools.partial(attend_body, blocks=blocks, heads=heads),
        in_specs=[pl.BlockSpec(memory_space=pltpu.SMEM)] + [vmem] * 4,
        out_specs=vmem,
        out_shape=jax.ShapeDtypeStruct((2, *qa.shape), jnp.bfloat16),
        scratch_shapes=[
            pltpu.VMEM((2, KEY_ROWS, columns), jnp.bfloat16),
            pltpu.VMEM((2, 1, columns), jnp.float32),
            pltpu.VMEM((2, VALUE_ROWS + 16, columns), jnp.float32),
        ],
        compiler_params=pltpu.CompilerParams(vmem_limit_bytes=48 * 1024 * 1024),
        name="attend_rows",
    )(index, qa, qb, own, other)


def routing(routes_ref, experts):
    rows = routes_ref.shape[0]
    lanes = lax.broadcasted_iota(jnp.int32, (rows, experts), 1)
    first = (routes_ref[:, 0:1] == lanes).astype(jnp.float32)
    second = (routes_ref[:, 1:2] == lanes).astype(jnp.float32)
    named = first + second
    above = lax.broadcasted_iota(jnp.int32, (rows, rows), 1) < lax.broadcasted_iota(
        jnp.int32, (rows, rows), 0
    )
    earlier = jnp.dot(
        above.astype(jnp.bfloat16), named.astype(jnp.bfloat16), preferred_element_type=jnp.float32
    )
    return first, second, named, earlier


def spread_rows(tiles_ref, rows, slot, capacity):
    count, width = rows.shape
    per_row = width // 128
    for j in range(per_row):
        at = pl.ds(slot * per_row + j, count, stride=capacity * per_row)
        tiles_ref[at, :] = rows[:, j * 128 : (j + 1) * 128]


def joined_rows(tiles_ref, slot, capacity, count, width):
    per_row = width // 128
    return jnp.concatenate(
        [
            tiles_ref[pl.ds(slot * per_row + j, count, stride=capacity * per_row), :]
            for j in range(per_row)
        ],
        axis=1,
    )


def dispatch_body(parts_ref, residual_ref, gain_ref, routes_ref, hidden_ref, slots_ref, tiles_ref, *, capacity):
    mixed = jnp.sum(parts_ref[...].astype(jnp.float32), axis=0)
    hidden = residual_ref[...].astype(jnp.float32) + mixed
    hidden_ref[...] = hidden
    scale = lax.rsqrt(jnp.mean(hidden * hidden, axis=1, keepdims=True) + NORM_EPS)
    normed = (hidden * scale * gain_ref[...]).astype(jnp.bfloat16)
    experts = slots_ref.shape[0]
    _, _, named, earlier = routing(routes_ref, experts)
    for slot in range(capacity):
        chosen = jnp.where(earlier == slot, named, 0.0).T.astype(jnp.bfloat16)
        spread_rows(
            tiles_ref,
            jnp.dot(chosen, normed, preferred_element_type=jnp.float32),
            slot,
            capacity,
        )
    slots_ref[...] = tiles_ref[...].reshape(slots_ref.shape).astype(jnp.bfloat16)


def dispatch(parts, residual, gain, routes, experts, capacity):
    rows, width = residual.shape
    return pl.pallas_call(
        functools.partial(dispatch_body, capacity=capacity),
        out_shape=[
            jax.ShapeDtypeStruct((rows, width), jnp.float32),
            jax.ShapeDtypeStruct((experts, capacity * width // 128, 128), jnp.bfloat16),
        ],
        scratch_shapes=[pltpu.VMEM((experts * capacity * width // 128, 128), jnp.float32)],
        name="dispatch",
    )(parts, residual, gain.reshape(1, width), routes)


def arrange_body(arrived_ref, rows_ref, tiles_ref, *, capacity):
    count = arrived_ref.shape[0]
    tiles_ref[...] = arrived_ref[...].astype(jnp.float32).reshape(tiles_ref.shape)
    for slot in range(capacity):
        rows_ref[slot * count : (slot + 1) * count, :] = joined_rows(
            tiles_ref, slot, capacity, count, rows_ref.shape[1]
        ).astype(jnp.bfloat16)


def arrange(arrived, capacity):
    count, lines, lanes = arrived.shape
    return pl.pallas_call(
        functools.partial(arrange_body, capacity=capacity),
        out_shape=jax.ShapeDtypeStruct((capacity * count, lines * lanes // capacity), jnp.bfloat16),
        scratch_shapes=[pltpu.VMEM((count * lines, lanes), jnp.float32)],
        name="arrange",
    )(arrived)


def spread_body(rows_ref, leaving_ref, tiles_ref, *, capacity):
    count = leaving_ref.shape[0]
    for slot in range(capacity):
        spread_rows(tiles_ref, rows_ref[slot * count : (slot + 1) * count, :], slot, capacity)
    leaving_ref[...] = tiles_ref[...].reshape(leaving_ref.shape).astype(jnp.bfloat16)


def spread(rows, capacity):
    count, width = rows.shape[0] // capacity, rows.shape[1]
    lines = capacity * width // 128
    return pl.pallas_call(
        functools.partial(spread_body, capacity=capacity),
        out_shape=jax.ShapeDtypeStruct((count, lines, 128), jnp.bfloat16),
        scratch_shapes=[pltpu.VMEM((count * lines, 128), jnp.float32)],
        name="spread",
    )(rows)


def combine_body(returned_ref, hidden_ref, routes_ref, weight_ref, out_ref, tiles_ref, *, capacity):
    experts = returned_ref.shape[0]
    tiles_ref[...] = returned_ref[...].astype(jnp.float32).reshape(tiles_ref.shape)
    first, second, _, earlier = routing(routes_ref, experts)
    weight = first * weight_ref[:, 0:1] + second * weight_ref[:, 1:2]
    total = hidden_ref[...]
    for slot in range(capacity):
        rest = jnp.where(earlier == slot, weight, 0.0)
        rows = joined_rows(tiles_ref, slot, capacity, experts, out_ref.shape[1]).astype(jnp.bfloat16)
        for _ in range(3):
            piece = rest.astype(jnp.bfloat16)
            rest = rest - piece.astype(jnp.float32)
            total = total + jnp.dot(piece, rows, preferred_element_type=jnp.float32)
    out_ref[...] = total.astype(jnp.bfloat16)


def combine(returned, hidden, routes, route_weight, capacity):
    experts, lines, lanes = returned.shape
    return pl.pallas_call(
        functools.partial(combine_body, capacity=capacity),
        out_shape=jax.ShapeDtypeStruct(hidden.shape, jnp.bfloat16),
        scratch_shapes=[pltpu.VMEM((experts * lines, lanes), jnp.float32)],
        name="combine",
    )(returned, hidden, routes, route_weight)


def layer(
    queries,
    key_value_pairs,
    forget_gate_total,
    residual_in,
    out_weight,
    norm_gain,
    routes,
    route_weight,
    expert_gate,
    expert_up,
    expert_down,
):
    seq_devices = lax.axis_size(SP)
    head_devices = lax.axis_size("tp")
    index = lax.axis_index(SP).astype(jnp.int32)
    mirror = [(i, seq_devices - 1 - i) for i in range(seq_devices)]
    up = [(i, (i + 1) % head_devices) for i in range(head_devices)]
    down = [(i, (i - 1) % head_devices) for i in range(head_devices)]

    def neighbours(array):
        return lax.ppermute(array, "tp", up), lax.ppermute(array, "tp", down)

    def opposite(before, after):
        half = before.shape[0] // 2
        return jnp.concatenate(
            [lax.ppermute(before[:half], "tp", up), lax.ppermute(after[half:], "tp", down)], axis=0
        )

    whole = [
        (i * head_devices + t, (i if 2 * t < head_devices else seq_devices - 1 - i) * head_devices + t)
        for i in range(seq_devices)
        for t in range(head_devices)
    ]
    flipped = 2 * lax.axis_index("tp") >= head_devices
    block = prepare_keys(key_value_pairs, forget_gate_total.T)
    mirrored_queries = lax.ppermute(queries[HALF:], SP, mirror)
    down_own = expert_down[0]
    down_before = lax.ppermute(down_own, "tp", up)
    down_after = lax.ppermute(down_own, "tp", down)
    near = lax.all_gather(block, "sp_1")
    near, mirrored_queries = lax.optimization_barrier((near, mirrored_queries))
    own = lax.all_gather(near, "sp_0").reshape(-1, *block.shape)
    own, swapped_residual, swapped_routes = lax.optimization_barrier((own, residual_in, routes))
    held_residual = lax.ppermute(swapped_residual, SP_TP, whole)
    held_routes = lax.ppermute(swapped_routes, SP_TP, whole)
    other = lax.ppermute(own, "sp_2", [(0, 1), (1, 0)])
    attended = attend_rows(
        index.reshape(1), queries[:HALF], mirrored_queries, own, other
    )
    down_before, down_after, attended, held_residual, held_routes = lax.optimization_barrier(
        (down_before, down_after, attended, held_residual, held_routes)
    )
    half = down_own.shape[0] // 2
    across_low = lax.ppermute(down_before[:half], "tp", up)
    across_high = lax.ppermute(down_after[half:], "tp", down)
    partial = jnp.dot(
        attended.reshape(-1, attended.shape[2]), out_weight, preferred_element_type=jnp.float32
    ).astype(jnp.bfloat16)
    parts = lax.all_to_all(
        partial.reshape(head_devices, -1, partial.shape[1]), "tp", 0, 0, tiled=True
    )
    own_rows, top_count = routes.shape
    capacity = max(2, 3 * own_rows * top_count // (2 * seq_devices))
    ranked_routes = jnp.where(flipped, seq_devices - 1 - held_routes, held_routes)
    held_hidden, slots = dispatch(
        parts, held_residual, norm_gain, ranked_routes, seq_devices, capacity
    )
    down_across = jnp.concatenate([across_low, across_high])
    ranks = [
        [(i if 2 * t < head_devices else seq_devices - 1 - i) * head_devices + t for i in range(seq_devices)]
        for t in range(head_devices)
    ]
    incoming = lax.all_to_all(
        slots, SP_TP, 0, 0, axis_index_groups=ranks, tiled=True
    )
    incoming, held_hidden = lax.optimization_barrier((incoming, held_hidden))
    hidden_state = lax.ppermute(held_hidden, SP_TP, whole)
    rows_own = arrange(incoming, capacity)

    def units(rows):
        gate_value = jnp.dot(rows, expert_gate[0], preferred_element_type=jnp.float32)
        up_value = jnp.dot(rows, expert_up[0], preferred_element_type=jnp.float32)
        return (jax.nn.silu(gate_value) * up_value).astype(jnp.bfloat16)

    rows_before, rows_after = neighbours(rows_own)
    units_own = units(rows_own)
    rows_across = opposite(rows_before, rows_after)
    rows_across, hidden_state = lax.optimization_barrier((rows_across, hidden_state))
    units_from_before = lax.ppermute(units(rows_after), "tp", up)
    units_from_after = lax.ppermute(units(rows_before), "tp", down)
    across = [(i, (i + 2) % head_devices) for i in range(head_devices)]
    units_from_across = lax.ppermute(units(rows_across), "tp", across)
    summed = jnp.dot(units_own, down_own, preferred_element_type=jnp.float32)
    for got, weight in (
        (units_from_before, down_before),
        (units_from_after, down_after),
        (units_from_across, down_across),
    ):
        summed = summed + jnp.dot(got, weight, preferred_element_type=jnp.float32)
    returned = lax.all_to_all(spread(summed, capacity), SP, 0, 0, tiled=True)
    return combine(returned, hidden_state, routes, route_weight, capacity)


def solution(mesh):
    finer = Mesh(mesh.devices.reshape(8, 4, 2, mesh.shape["tp"]), ("sp_0", "sp_1", "sp_2", "tp"))
    in_specs = (
        P(SP, "tp"),
        P(SP, "tp"),
        P(SP, "tp"),
        P(SP_TP, None),
        P("tp", None),
        P(),
        P(SP_TP, None),
        P(SP_TP, None),
        P(SP, None, "tp"),
        P(SP, None, "tp"),
        P(SP, "tp", None),
    )
    out_specs = P(SP_TP, None)
    return jax.shard_map(layer, mesh=finer, in_specs=in_specs, out_specs=out_specs, check_vma=False)
```

```python
import functools
import math

import jax
import jax.numpy as jnp
from jax import lax
from jax.experimental import pallas as pl
from jax.experimental.pallas import tpu as pltpu
from jax.sharding import Mesh
from jax.sharding import PartitionSpec as P

SP = ("sp_0", "sp_1", "sp_2")
SP_TP = ("sp_0", "sp_1", "sp_2", "tp")
NORM_EPS = 1e-06
HEAD_SIZE = 64
NEG_FILL = -1e30
LOG2E = math.log2(math.e)
BLOCK = 256
HALF = 128
KEY_ROWS = 96
VALUE_ROWS = 64


SAFE_SCORE = 60.0
STEP = 512
PAIRS = 2


def bf16_pieces(values):
    high = values.astype(jnp.bfloat16).astype(jnp.float32)
    rest = values - high
    middle = rest.astype(jnp.bfloat16).astype(jnp.float32)
    return [high, middle, rest - middle]


def prep_body(kv_ref, gate_ref, out_ref):
    kv = kv_ref[...].astype(jnp.float32).T
    keys = kv[:HEAD_SIZE]
    square = jnp.sum(keys * keys, axis=0, keepdims=True) * 1.02
    ones = jnp.ones_like(square)
    zeros = jnp.zeros_like(square)
    out_ref[...] = jnp.concatenate(
        [keys, *bf16_pieces(gate_ref[...])] + [ones] * 3 + [square] + [zeros] * 4 + [kv[HEAD_SIZE:]],
        axis=0,
    ).astype(jnp.bfloat16)


def prepare_keys(kv, gate_t):
    return pl.pallas_call(
        prep_body,
        out_shape=jax.ShapeDtypeStruct((KEY_ROWS + VALUE_ROWS, kv.shape[0]), jnp.bfloat16),
        name="prepare_keys",
    )(kv, gate_t)


def attend_body(index_ref, qa_ref, qb_ref, own_ref, other_ref, out_ref, qt_ref, max_ref, acc_ref, *, blocks, heads):
    columns = heads * HALF
    step = STEP
    own_index = index_ref[0]
    core = own_index % 2
    picked = 3 * heads
    row = lax.broadcasted_iota(jnp.int32, (picked, columns), 0)
    head = lax.broadcasted_iota(jnp.int32, (picked, columns), 1) // HALF
    picks = jnp.where(row % heads == head, -1.0, 0.0)
    largest_query = jnp.float32(0.0)
    mirror = blocks - 1 - own_index
    gates_at = slice(HEAD_SIZE, HEAD_SIZE + picked)
    gates_a = own_ref[own_index // 2, gates_at, :HALF].astype(jnp.float32)
    gates_b = other_ref[mirror // 2, gates_at, HALF:].astype(jnp.float32)
    for which, q_ref, gates in ((0, qa_ref, gates_a), (1, qb_ref, gates_b)):
        qt = (q_ref[...].astype(jnp.float32) * (HEAD_SIZE**-0.5)).T
        qt = jnp.concatenate(
            [qt[h * HEAD_SIZE : (h + 1) * HEAD_SIZE] for h in range(heads)], axis=1
        )
        largest_query = jnp.maximum(
            largest_query, jnp.max(jnp.sum(qt * qt, axis=0, keepdims=True))
        )
        pieces = [
            jnp.concatenate([gates[p + h : p + h + 1] for h in range(heads)], axis=1)
            for p in range(0, picked, heads)
        ]
        qt_ref[which] = jnp.concatenate(
            [qt, picks, *pieces, jnp.zeros((5, columns), jnp.float32)], axis=0
        ).astype(jnp.bfloat16)
    tail = slice(KEY_ROWS - 16, KEY_ROWS)
    squares = jnp.maximum(
        jnp.max(own_ref[:, tail].astype(jnp.float32), axis=0),
        jnp.max(other_ref[:, tail].astype(jnp.float32), axis=0),
    )
    largest_key = jnp.max(squares[11:12])
    bounded = largest_query * largest_key <= SAFE_SCORE**2
    acc_ref[...] = jnp.zeros(acc_ref.shape, jnp.float32)

    def operands(pair, count=1):
        tile = jnp.concatenate(
            [r[pair + n] for n in range(count) for r in (own_ref, other_ref)], axis=1
        )
        keys = tile[:KEY_ROWS].astype(jnp.float32).T.astype(jnp.bfloat16)
        values = jnp.concatenate(
            [tile[KEY_ROWS:], jnp.ones((16, tile.shape[1]), jnp.bfloat16)], axis=0
        )
        return keys, values

    def masked(scores, pair, first_row):
        k = lax.broadcasted_iota(jnp.int32, scores.shape, 0)
        t = lax.broadcasted_iota(jnp.int32, scores.shape, 1) % HALF
        start = jnp.where(k < BLOCK, core * BLOCK, (1 - core) * BLOCK - BLOCK)
        seen = pair * (2 * BLOCK) + start + k <= first_row + t
        return jnp.where(seen, scores, NEG_FILL)

    def plan(which):
        index = jnp.where(which == 0, own_index, blocks - 1 - own_index)
        return index // 2, index * BLOCK + which * HALF

    def plain(which, pair, first_row, count=1):
        keys, values = operands(pair, count)
        for at in range(0, columns, step):
            cols = slice(at, at + step)
            scores = jnp.dot(keys, qt_ref[which, :, cols], preferred_element_type=jnp.float32)
            if first_row is not None:
                scores = masked(scores, pair, first_row)
            weights = jnp.exp2(scores * LOG2E).astype(jnp.bfloat16)
            acc_ref[which, :, cols] += jnp.dot(values, weights, preferred_element_type=jnp.float32)

    def shifted(which, pair, first_row):
        keys, values = operands(pair)

        def chunk(c, carry):
            cols = pl.ds(pl.multiple_of(c * step, step), step)
            scores = jnp.dot(keys, qt_ref[which, :, cols], preferred_element_type=jnp.float32)
            scores = masked(scores, pair, first_row)
            before = max_ref[which, :, cols]
            now = jnp.maximum(before, jnp.max(scores, axis=0, keepdims=True))
            weights = jnp.exp2((scores - now) * LOG2E)
            rescale = jnp.exp2((before - now) * LOG2E)
            max_ref[which, :, cols] = now
            acc_ref[which, :, cols] = acc_ref[which, :, cols] * rescale + jnp.dot(
                values, weights.astype(jnp.bfloat16), preferred_element_type=jnp.float32
            )
            return carry

        lax.fori_loop(0, columns // step, chunk, 0)

    @pl.when(bounded)
    def _():
        def one(which, carry):
            last_pair, first_row = plan(which)

            def full(pair, inner):
                plain(which, pair, None)
                return inner

            def many(group, inner):
                plain(which, group * PAIRS, None, PAIRS)
                return inner

            groups = last_pair // PAIRS
            if PAIRS > 1:
                lax.fori_loop(0, groups, many, 0)
                lax.fori_loop(groups * PAIRS, last_pair, full, 0)
            else:
                lax.fori_loop(0, last_pair, full, 0)
            plain(which, last_pair, first_row)
            return carry

        lax.fori_loop(0, 2, one, 0)

    @pl.when(jnp.logical_not(bounded))
    def _():
        max_ref[...] = jnp.full(max_ref.shape, NEG_FILL, jnp.float32)

        def one(which, carry):
            last_pair, first_row = plan(which)

            def any_pair(pair, inner):
                shifted(which, pair, first_row)
                return inner

            lax.fori_loop(0, last_pair + 1, any_pair, 0)
            return carry

        lax.fori_loop(0, 2, one, 0)

    for which in range(2):
        acc = acc_ref[which]
        out = acc[:VALUE_ROWS] / acc[VALUE_ROWS : VALUE_ROWS + 1]
        out = jnp.concatenate([out[:, h * HALF : (h + 1) * HALF] for h in range(heads)], axis=0)
        out_ref[which] = out.T.astype(out_ref.dtype)


def attend_rows(index, qa, qb, own, other):
    heads = qa.shape[1] // HEAD_SIZE
    blocks = 2 * own.shape[0]
    columns = heads * HALF
    vmem = pl.BlockSpec(memory_space=pltpu.VMEM)
    return pl.pallas_call(
        functools.partial(attend_body, blocks=blocks, heads=heads),
        in_specs=[pl.BlockSpec(memory_space=pltpu.SMEM)] + [vmem] * 4,
        out_specs=vmem,
        out_shape=jax.ShapeDtypeStruct((2, *qa.shape), jnp.bfloat16),
        scratch_shapes=[
            pltpu.VMEM((2, KEY_ROWS, columns), jnp.bfloat16),
            pltpu.VMEM((2, 1, columns), jnp.float32),
            pltpu.VMEM((2, VALUE_ROWS + 16, columns), jnp.float32),
        ],
        compiler_params=pltpu.CompilerParams(vmem_limit_bytes=48 * 1024 * 1024),
        name="attend_rows",
    )(index, qa, qb, own, other)


def routing(routes_ref, experts):
    rows = routes_ref.shape[0]
    lanes = lax.broadcasted_iota(jnp.int32, (rows, experts), 1)
    first = (routes_ref[:, 0:1] == lanes).astype(jnp.float32)
    second = (routes_ref[:, 1:2] == lanes).astype(jnp.float32)
    named = first + second
    above = lax.broadcasted_iota(jnp.int32, (rows, rows), 1) < lax.broadcasted_iota(
        jnp.int32, (rows, rows), 0
    )
    earlier = jnp.dot(
        above.astype(jnp.bfloat16), named.astype(jnp.bfloat16), preferred_element_type=jnp.float32
    )
    return first, second, named, earlier


def spread_rows(tiles_ref, rows, slot, capacity):
    count, width = rows.shape
    per_row = width // 128
    for j in range(per_row):
        at = pl.ds(slot * per_row + j, count, stride=capacity * per_row)
        tiles_ref[at, :] = rows[:, j * 128 : (j + 1) * 128]


def joined_rows(tiles_ref, slot, capacity, count, width):
    per_row = width // 128
    return jnp.concatenate(
        [
            tiles_ref[pl.ds(slot * per_row + j, count, stride=capacity * per_row), :]
            for j in range(per_row)
        ],
        axis=1,
    )


def dispatch_body(parts_ref, residual_ref, gain_ref, routes_ref, hidden_ref, slots_ref, tiles_ref, *, capacity):
    mixed = jnp.sum(parts_ref[...].astype(jnp.float32), axis=0)
    hidden = residual_ref[...].astype(jnp.float32) + mixed
    hidden_ref[...] = hidden
    scale = lax.rsqrt(jnp.mean(hidden * hidden, axis=1, keepdims=True) + NORM_EPS)
    normed = (hidden * scale * gain_ref[...]).astype(jnp.bfloat16)
    experts = slots_ref.shape[0]
    _, _, named, earlier = routing(routes_ref, experts)
    for slot in range(capacity):
        chosen = jnp.where(earlier == slot, named, 0.0).T.astype(jnp.bfloat16)
        spread_rows(
            tiles_ref,
            jnp.dot(chosen, normed, preferred_element_type=jnp.float32),
            slot,
            capacity,
        )
    slots_ref[...] = tiles_ref[...].reshape(slots_ref.shape).astype(jnp.bfloat16)


def dispatch(parts, residual, gain, routes, experts, capacity):
    rows, width = residual.shape
    return pl.pallas_call(
        functools.partial(dispatch_body, capacity=capacity),
        out_shape=[
            jax.ShapeDtypeStruct((rows, width), jnp.float32),
            jax.ShapeDtypeStruct((experts, capacity * width // 128, 128), jnp.bfloat16),
        ],
        scratch_shapes=[pltpu.VMEM((experts * capacity * width // 128, 128), jnp.float32)],
        name="dispatch",
    )(parts, residual, gain.reshape(1, width), routes)


def arrange_body(arrived_ref, rows_ref, tiles_ref, *, capacity):
    count = arrived_ref.shape[0]
    tiles_ref[...] = arrived_ref[...].astype(jnp.float32).reshape(tiles_ref.shape)
    for slot in range(capacity):
        rows_ref[slot * count : (slot + 1) * count, :] = joined_rows(
            tiles_ref, slot, capacity, count, rows_ref.shape[1]
        ).astype(jnp.bfloat16)


def arrange(arrived, capacity):
    count, lines, lanes = arrived.shape
    return pl.pallas_call(
        functools.partial(arrange_body, capacity=capacity),
        out_shape=jax.ShapeDtypeStruct((capacity * count, lines * lanes // capacity), jnp.bfloat16),
        scratch_shapes=[pltpu.VMEM((count * lines, lanes), jnp.float32)],
        name="arrange",
    )(arrived)


def spread_body(rows_ref, leaving_ref, tiles_ref, *, capacity):
    count = leaving_ref.shape[0]
    for slot in range(capacity):
        spread_rows(tiles_ref, rows_ref[slot * count : (slot + 1) * count, :], slot, capacity)
    leaving_ref[...] = tiles_ref[...].reshape(leaving_ref.shape).astype(jnp.bfloat16)


def spread(rows, capacity):
    count, width = rows.shape[0] // capacity, rows.shape[1]
    lines = capacity * width // 128
    return pl.pallas_call(
        functools.partial(spread_body, capacity=capacity),
        out_shape=jax.ShapeDtypeStruct((count, lines, 128), jnp.bfloat16),
        scratch_shapes=[pltpu.VMEM((count * lines, 128), jnp.float32)],
        name="spread",
    )(rows)


def combine_body(returned_ref, hidden_ref, routes_ref, weight_ref, out_ref, tiles_ref, *, capacity):
    experts = returned_ref.shape[0]
    tiles_ref[...] = returned_ref[...].astype(jnp.float32).reshape(tiles_ref.shape)
    first, second, _, earlier = routing(routes_ref, experts)
    weight = first * weight_ref[:, 0:1] + second * weight_ref[:, 1:2]
    total = hidden_ref[...]
    for slot in range(capacity):
        rest = jnp.where(earlier == slot, weight, 0.0)
        rows = joined_rows(tiles_ref, slot, capacity, experts, out_ref.shape[1]).astype(jnp.bfloat16)
        for _ in range(3):
            piece = rest.astype(jnp.bfloat16)
            rest = rest - piece.astype(jnp.float32)
            total = total + jnp.dot(piece, rows, preferred_element_type=jnp.float32)
    out_ref[...] = total.astype(jnp.bfloat16)


def combine(returned, hidden, routes, route_weight, capacity):
    experts, lines, lanes = returned.shape
    return pl.pallas_call(
        functools.partial(combine_body, capacity=capacity),
        out_shape=jax.ShapeDtypeStruct(hidden.shape, jnp.bfloat16),
        scratch_shapes=[pltpu.VMEM((experts * lines, lanes), jnp.float32)],
        name="combine",
    )(returned, hidden, routes, route_weight)


def layer(
    queries,
    key_value_pairs,
    forget_gate_total,
    residual_in,
    out_weight,
    norm_gain,
    routes,
    route_weight,
    expert_gate,
    expert_up,
    expert_down,
):
    seq_devices = lax.axis_size(SP)
    head_devices = lax.axis_size("tp")
    index = lax.axis_index(SP).astype(jnp.int32)
    mirror = [(i, seq_devices - 1 - i) for i in range(seq_devices)]
    up = [(i, (i + 1) % head_devices) for i in range(head_devices)]
    down = [(i, (i - 1) % head_devices) for i in range(head_devices)]

    def neighbours(array):
        return lax.ppermute(array, "tp", up), lax.ppermute(array, "tp", down)

    def opposite(before, after):
        half = before.shape[0] // 2
        return jnp.concatenate(
            [lax.ppermute(before[:half], "tp", up), lax.ppermute(after[half:], "tp", down)], axis=0
        )

    whole = [
        (i * head_devices + t, (i if 2 * t < head_devices else seq_devices - 1 - i) * head_devices + t)
        for i in range(seq_devices)
        for t in range(head_devices)
    ]
    flipped = 2 * lax.axis_index("tp") >= head_devices
    block = prepare_keys(key_value_pairs, forget_gate_total.T)
    mirrored_queries = lax.ppermute(queries[HALF:], SP, mirror)
    down_own = expert_down[0]
    down_before = lax.ppermute(down_own, "tp", up)
    down_after = lax.ppermute(down_own, "tp", down)
    held_residual = lax.ppermute(residual_in, SP_TP, whole)
    held_routes = lax.ppermute(routes, SP_TP, whole)
    near = lax.all_gather(block, "sp_1")
    near, mirrored_queries = lax.optimization_barrier((near, mirrored_queries))
    own = lax.all_gather(near, "sp_0").reshape(-1, *block.shape)
    own, held_residual, held_routes = lax.optimization_barrier((own, held_residual, held_routes))
    other = lax.ppermute(own, "sp_2", [(0, 1), (1, 0)])
    attended = attend_rows(
        index.reshape(1), queries[:HALF], mirrored_queries, own, other
    )
    down_before, down_after, attended = lax.optimization_barrier(
        (down_before, down_after, attended)
    )
    half = down_own.shape[0] // 2
    across_low = lax.ppermute(down_before[:half], "tp", up)
    across_high = lax.ppermute(down_after[half:], "tp", down)
    partial = jnp.dot(
        attended.reshape(-1, attended.shape[2]), out_weight, preferred_element_type=jnp.float32
    ).astype(jnp.bfloat16)
    parts = lax.all_to_all(
        partial.reshape(head_devices, -1, partial.shape[1]), "tp", 0, 0, tiled=True
    )
    own_rows, top_count = routes.shape
    capacity = max(2, 3 * own_rows * top_count // (2 * seq_devices))
    ranked_routes = jnp.where(flipped, seq_devices - 1 - held_routes, held_routes)
    held_hidden, slots = dispatch(
        parts, held_residual, norm_gain, ranked_routes, seq_devices, capacity
    )
    down_across = jnp.concatenate([across_low, across_high])
    ranks = [
        [(i if 2 * t < head_devices else seq_devices - 1 - i) * head_devices + t for i in range(seq_devices)]
        for t in range(head_devices)
    ]
    incoming = lax.all_to_all(
        slots, SP_TP, 0, 0, axis_index_groups=ranks, tiled=True
    )
    incoming, held_hidden = lax.optimization_barrier((incoming, held_hidden))
    hidden_state = lax.ppermute(held_hidden, SP_TP, whole)
    rows_own = arrange(incoming, capacity)

    def units(rows):
        gate_value = jnp.dot(rows, expert_gate[0], preferred_element_type=jnp.float32)
        up_value = jnp.dot(rows, expert_up[0], preferred_element_type=jnp.float32)
        return (jax.nn.silu(gate_value) * up_value).astype(jnp.bfloat16)

    rows_before, rows_after = neighbours(rows_own)
    units_own = units(rows_own)
    rows_across = opposite(rows_before, rows_after)
    rows_across, hidden_state = lax.optimization_barrier((rows_across, hidden_state))
    units_from_before = lax.ppermute(units(rows_after), "tp", up)
    units_from_after = lax.ppermute(units(rows_before), "tp", down)
    across = [(i, (i + 2) % head_devices) for i in range(head_devices)]
    units_from_across = lax.ppermute(units(rows_across), "tp", across)
    summed = jnp.dot(units_own, down_own, preferred_element_type=jnp.float32)
    for got, weight in (
        (units_from_before, down_before),
        (units_from_after, down_after),
        (units_from_across, down_across),
    ):
        summed = summed + jnp.dot(got, weight, preferred_element_type=jnp.float32)
    returned = lax.all_to_all(spread(summed, capacity), SP, 0, 0, tiled=True)
    return combine(returned, hidden_state, routes, route_weight, capacity)


def solution(mesh):
    finer = Mesh(mesh.devices.reshape(8, 4, 2, mesh.shape["tp"]), ("sp_0", "sp_1", "sp_2", "tp"))
    in_specs = (
        P(SP, "tp"),
        P(SP, "tp"),
        P(SP, "tp"),
        P(SP_TP, None),
        P("tp", None),
        P(),
        P(SP_TP, None),
        P(SP_TP, None),
        P(SP, None, "tp"),
        P(SP, None, "tp"),
        P(SP, "tp", None),
    )
    out_specs = P(SP_TP, None)
    return jax.shard_map(layer, mesh=finer, in_specs=in_specs, out_specs=out_specs, check_vma=False)
```

```python
import functools
import math

import jax
import jax.numpy as jnp
from jax import lax
from jax.experimental import pallas as pl
from jax.experimental.pallas import tpu as pltpu
from jax.sharding import Mesh
from jax.sharding import PartitionSpec as P

SP = ("sp_0", "sp_1", "sp_2")
SP_TP = ("sp_0", "sp_1", "sp_2", "tp")
NORM_EPS = 1e-06
HEAD_SIZE = 64
NEG_FILL = -1e30
LOG2E = math.log2(math.e)
BLOCK = 256
HALF = 128
KEY_ROWS = 96
VALUE_ROWS = 64


SAFE_SCORE = 60.0
STEP = 512
PAIRS = 2


def bf16_pieces(values):
    high = values.astype(jnp.bfloat16).astype(jnp.float32)
    rest = values - high
    middle = rest.astype(jnp.bfloat16).astype(jnp.float32)
    return [high, middle, rest - middle]


def prep_body(kv_ref, gate_ref, out_ref):
    kv = kv_ref[...].astype(jnp.float32).T
    keys = kv[:HEAD_SIZE]
    square = jnp.sum(keys * keys, axis=0, keepdims=True) * 1.02
    ones = jnp.ones_like(square)
    zeros = jnp.zeros_like(square)
    out_ref[...] = jnp.concatenate(
        [keys, *bf16_pieces(gate_ref[...])] + [ones] * 3 + [square] + [zeros] * 4 + [kv[HEAD_SIZE:]],
        axis=0,
    ).astype(jnp.bfloat16)


def prepare_keys(kv, gate_t):
    return pl.pallas_call(
        prep_body,
        out_shape=jax.ShapeDtypeStruct((KEY_ROWS + VALUE_ROWS, kv.shape[0]), jnp.bfloat16),
        name="prepare_keys",
    )(kv, gate_t)


def attend_body(index_ref, qa_ref, qb_ref, own_ref, other_ref, out_ref, qt_ref, max_ref, acc_ref, *, blocks, heads):
    columns = heads * HALF
    step = STEP
    own_index = index_ref[0]
    core = own_index % 2
    picked = 3 * heads
    row = lax.broadcasted_iota(jnp.int32, (picked, columns), 0)
    head = lax.broadcasted_iota(jnp.int32, (picked, columns), 1) // HALF
    picks = jnp.where(row % heads == head, -1.0, 0.0)
    largest_query = jnp.float32(0.0)
    mirror = blocks - 1 - own_index
    gates_at = slice(HEAD_SIZE, HEAD_SIZE + picked)
    gates_a = own_ref[own_index // 2, gates_at, :HALF].astype(jnp.float32)
    gates_b = other_ref[mirror // 2, gates_at, HALF:].astype(jnp.float32)
    for which, q_ref, gates in ((0, qa_ref, gates_a), (1, qb_ref, gates_b)):
        qt = (q_ref[...].astype(jnp.float32) * (HEAD_SIZE**-0.5)).T
        qt = jnp.concatenate(
            [qt[h * HEAD_SIZE : (h + 1) * HEAD_SIZE] for h in range(heads)], axis=1
        )
        largest_query = jnp.maximum(
            largest_query, jnp.max(jnp.sum(qt * qt, axis=0, keepdims=True))
        )
        pieces = [
            jnp.concatenate([gates[p + h : p + h + 1] for h in range(heads)], axis=1)
            for p in range(0, picked, heads)
        ]
        qt_ref[which] = jnp.concatenate(
            [qt, picks, *pieces, jnp.zeros((5, columns), jnp.float32)], axis=0
        ).astype(jnp.bfloat16)
    tail = slice(KEY_ROWS - 16, KEY_ROWS)
    squares = jnp.maximum(
        jnp.max(own_ref[:, tail].astype(jnp.float32), axis=0),
        jnp.max(other_ref[:, tail].astype(jnp.float32), axis=0),
    )
    largest_key = jnp.max(squares[11:12])
    bounded = largest_query * largest_key <= SAFE_SCORE**2
    acc_ref[...] = jnp.zeros(acc_ref.shape, jnp.float32)

    def operands(pair, count=1):
        tile = jnp.concatenate(
            [r[pair + n] for n in range(count) for r in (own_ref, other_ref)], axis=1
        )
        keys = tile[:KEY_ROWS].astype(jnp.float32).T.astype(jnp.bfloat16)
        values = jnp.concatenate(
            [tile[KEY_ROWS:], jnp.ones((16, tile.shape[1]), jnp.bfloat16)], axis=0
        )
        return keys, values

    def masked(scores, pair, first_row):
        k = lax.broadcasted_iota(jnp.int32, scores.shape, 0)
        t = lax.broadcasted_iota(jnp.int32, scores.shape, 1) % HALF
        start = jnp.where(k < BLOCK, core * BLOCK, (1 - core) * BLOCK - BLOCK)
        seen = pair * (2 * BLOCK) + start + k <= first_row + t
        return jnp.where(seen, scores, NEG_FILL)

    def plan(which):
        index = jnp.where(which == 0, own_index, blocks - 1 - own_index)
        return index // 2, index * BLOCK + which * HALF

    def plain(which, pair, first_row, count=1):
        keys, values = operands(pair, count)
        for at in range(0, columns, step):
            cols = slice(at, at + step)
            scores = jnp.dot(keys, qt_ref[which, :, cols], preferred_element_type=jnp.float32)
            if first_row is not None:
                scores = masked(scores, pair, first_row)
            weights = jnp.exp2(scores * LOG2E).astype(jnp.bfloat16)
            acc_ref[which, :, cols] += jnp.dot(values, weights, preferred_element_type=jnp.float32)

    def shifted(which, pair, first_row):
        keys, values = operands(pair)

        def chunk(c, carry):
            cols = pl.ds(pl.multiple_of(c * step, step), step)
            scores = jnp.dot(keys, qt_ref[which, :, cols], preferred_element_type=jnp.float32)
            scores = masked(scores, pair, first_row)
            before = max_ref[which, :, cols]
            now = jnp.maximum(before, jnp.max(scores, axis=0, keepdims=True))
            weights = jnp.exp2((scores - now) * LOG2E)
            rescale = jnp.exp2((before - now) * LOG2E)
            max_ref[which, :, cols] = now
            acc_ref[which, :, cols] = acc_ref[which, :, cols] * rescale + jnp.dot(
                values, weights.astype(jnp.bfloat16), preferred_element_type=jnp.float32
            )
            return carry

        lax.fori_loop(0, columns // step, chunk, 0)

    @pl.when(bounded)
    def _():
        def one(which, carry):
            last_pair, first_row = plan(which)

            def full(pair, inner):
                plain(which, pair, None)
                return inner

            def many(group, inner):
                plain(which, group * PAIRS, None, PAIRS)
                return inner

            groups = last_pair // PAIRS
            if PAIRS > 1:
                lax.fori_loop(0, groups, many, 0)
                lax.fori_loop(groups * PAIRS, last_pair, full, 0)
            else:
                lax.fori_loop(0, last_pair, full, 0)
            plain(which, last_pair, first_row)
            return carry

        lax.fori_loop(0, 2, one, 0)

    @pl.when(jnp.logical_not(bounded))
    def _():
        max_ref[...] = jnp.full(max_ref.shape, NEG_FILL, jnp.float32)

        def one(which, carry):
            last_pair, first_row = plan(which)

            def any_pair(pair, inner):
                shifted(which, pair, first_row)
                return inner

            lax.fori_loop(0, last_pair + 1, any_pair, 0)
            return carry

        lax.fori_loop(0, 2, one, 0)

    for which in range(2):
        acc = acc_ref[which]
        out = acc[:VALUE_ROWS] / acc[VALUE_ROWS : VALUE_ROWS + 1]
        out = jnp.concatenate([out[:, h * HALF : (h + 1) * HALF] for h in range(heads)], axis=0)
        out_ref[which] = out.T.astype(out_ref.dtype)


def attend_rows(index, qa, qb, own, other):
    heads = qa.shape[1] // HEAD_SIZE
    blocks = 2 * own.shape[0]
    columns = heads * HALF
    vmem = pl.BlockSpec(memory_space=pltpu.VMEM)
    return pl.pallas_call(
        functools.partial(attend_body, blocks=blocks, heads=heads),
        in_specs=[pl.BlockSpec(memory_space=pltpu.SMEM)] + [vmem] * 4,
        out_specs=vmem,
        out_shape=jax.ShapeDtypeStruct((2, *qa.shape), jnp.bfloat16),
        scratch_shapes=[
            pltpu.VMEM((2, KEY_ROWS, columns), jnp.bfloat16),
            pltpu.VMEM((2, 1, columns), jnp.float32),
            pltpu.VMEM((2, VALUE_ROWS + 16, columns), jnp.float32),
        ],
        compiler_params=pltpu.CompilerParams(vmem_limit_bytes=48 * 1024 * 1024),
        name="attend_rows",
    )(index, qa, qb, own, other)


def routing(routes_ref, experts):
    rows = routes_ref.shape[0]
    lanes = lax.broadcasted_iota(jnp.int32, (rows, experts), 1)
    first = (routes_ref[:, 0:1] == lanes).astype(jnp.float32)
    second = (routes_ref[:, 1:2] == lanes).astype(jnp.float32)
    named = first + second
    above = lax.broadcasted_iota(jnp.int32, (rows, rows), 1) < lax.broadcasted_iota(
        jnp.int32, (rows, rows), 0
    )
    earlier = jnp.dot(
        above.astype(jnp.bfloat16), named.astype(jnp.bfloat16), preferred_element_type=jnp.float32
    )
    return first, second, named, earlier


def spread_rows(tiles_ref, rows, slot, capacity):
    count, width = rows.shape
    per_row = width // 128
    for j in range(per_row):
        at = pl.ds(slot * per_row + j, count, stride=capacity * per_row)
        tiles_ref[at, :] = rows[:, j * 128 : (j + 1) * 128]


def joined_rows(tiles_ref, slot, capacity, count, width):
    per_row = width // 128
    return jnp.concatenate(
        [
            tiles_ref[pl.ds(slot * per_row + j, count, stride=capacity * per_row), :]
            for j in range(per_row)
        ],
        axis=1,
    )


def dispatch_body(parts_ref, residual_ref, gain_ref, routes_ref, hidden_ref, slots_ref, tiles_ref, *, capacity):
    mixed = jnp.sum(parts_ref[...].astype(jnp.float32), axis=0)
    hidden = residual_ref[...].astype(jnp.float32) + mixed
    hidden_ref[...] = hidden
    scale = lax.rsqrt(jnp.mean(hidden * hidden, axis=1, keepdims=True) + NORM_EPS)
    normed = (hidden * scale * gain_ref[...]).astype(jnp.bfloat16)
    experts = slots_ref.shape[0]
    _, _, named, earlier = routing(routes_ref, experts)
    for slot in range(capacity):
        chosen = jnp.where(earlier == slot, named, 0.0).T.astype(jnp.bfloat16)
        spread_rows(
            tiles_ref,
            jnp.dot(chosen, normed, preferred_element_type=jnp.float32),
            slot,
            capacity,
        )
    slots_ref[...] = tiles_ref[...].reshape(slots_ref.shape).astype(jnp.bfloat16)


def dispatch(parts, residual, gain, routes, experts, capacity):
    rows, width = residual.shape
    return pl.pallas_call(
        functools.partial(dispatch_body, capacity=capacity),
        out_shape=[
            jax.ShapeDtypeStruct((rows, width), jnp.float32),
            jax.ShapeDtypeStruct((experts, capacity * width // 128, 128), jnp.bfloat16),
        ],
        scratch_shapes=[pltpu.VMEM((experts * capacity * width // 128, 128), jnp.float32)],
        name="dispatch",
    )(parts, residual, gain.reshape(1, width), routes)


def arrange_body(arrived_ref, rows_ref, tiles_ref, *, capacity):
    count = arrived_ref.shape[0]
    tiles_ref[...] = arrived_ref[...].astype(jnp.float32).reshape(tiles_ref.shape)
    for slot in range(capacity):
        rows_ref[slot * count : (slot + 1) * count, :] = joined_rows(
            tiles_ref, slot, capacity, count, rows_ref.shape[1]
        ).astype(jnp.bfloat16)


def arrange(arrived, capacity):
    count, lines, lanes = arrived.shape
    return pl.pallas_call(
        functools.partial(arrange_body, capacity=capacity),
        out_shape=jax.ShapeDtypeStruct((capacity * count, lines * lanes // capacity), jnp.bfloat16),
        scratch_shapes=[pltpu.VMEM((count * lines, lanes), jnp.float32)],
        name="arrange",
    )(arrived)


def spread_body(rows_ref, leaving_ref, tiles_ref, *, capacity):
    count = leaving_ref.shape[0]
    for slot in range(capacity):
        spread_rows(tiles_ref, rows_ref[slot * count : (slot + 1) * count, :], slot, capacity)
    leaving_ref[...] = tiles_ref[...].reshape(leaving_ref.shape).astype(jnp.bfloat16)


def spread(rows, capacity):
    count, width = rows.shape[0] // capacity, rows.shape[1]
    lines = capacity * width // 128
    return pl.pallas_call(
        functools.partial(spread_body, capacity=capacity),
        out_shape=jax.ShapeDtypeStruct((count, lines, 128), jnp.bfloat16),
        scratch_shapes=[pltpu.VMEM((count * lines, 128), jnp.float32)],
        name="spread",
    )(rows)


def combine_body(returned_ref, hidden_ref, routes_ref, weight_ref, out_ref, tiles_ref, *, capacity):
    experts = returned_ref.shape[0]
    tiles_ref[...] = returned_ref[...].astype(jnp.float32).reshape(tiles_ref.shape)
    first, second, _, earlier = routing(routes_ref, experts)
    weight = first * weight_ref[:, 0:1] + second * weight_ref[:, 1:2]
    total = hidden_ref[...]
    for slot in range(capacity):
        rest = jnp.where(earlier == slot, weight, 0.0)
        rows = joined_rows(tiles_ref, slot, capacity, experts, out_ref.shape[1]).astype(jnp.bfloat16)
        for _ in range(3):
            piece = rest.astype(jnp.bfloat16)
            rest = rest - piece.astype(jnp.float32)
            total = total + jnp.dot(piece, rows, preferred_element_type=jnp.float32)
    out_ref[...] = total.astype(jnp.bfloat16)


def combine(returned, hidden, routes, route_weight, capacity):
    experts, lines, lanes = returned.shape
    return pl.pallas_call(
        functools.partial(combine_body, capacity=capacity),
        out_shape=jax.ShapeDtypeStruct(hidden.shape, jnp.bfloat16),
        scratch_shapes=[pltpu.VMEM((experts * lines, lanes), jnp.float32)],
        name="combine",
    )(returned, hidden, routes, route_weight)


def layer(
    queries,
    key_value_pairs,
    forget_gate_total,
    residual_in,
    out_weight,
    norm_gain,
    routes,
    route_weight,
    expert_gate,
    expert_up,
    expert_down,
):
    seq_devices = lax.axis_size(SP)
    head_devices = lax.axis_size("tp")
    index = lax.axis_index(SP).astype(jnp.int32)
    mirror = [(i, seq_devices - 1 - i) for i in range(seq_devices)]
    up = [(i, (i + 1) % head_devices) for i in range(head_devices)]
    down = [(i, (i - 1) % head_devices) for i in range(head_devices)]

    def neighbours(array):
        return lax.ppermute(array, "tp", up), lax.ppermute(array, "tp", down)

    def opposite(before, after):
        half = before.shape[0] // 2
        return jnp.concatenate(
            [lax.ppermute(before[:half], "tp", up), lax.ppermute(after[half:], "tp", down)], axis=0
        )

    whole = [
        (i * head_devices + t, (i if 2 * t < head_devices else seq_devices - 1 - i) * head_devices + t)
        for i in range(seq_devices)
        for t in range(head_devices)
    ]
    flipped = 2 * lax.axis_index("tp") >= head_devices
    block = prepare_keys(key_value_pairs, forget_gate_total.T)
    mirrored_queries = lax.ppermute(queries[HALF:], SP, mirror)
    down_own = expert_down[0]
    down_before = lax.ppermute(down_own, "tp", up)
    down_after = lax.ppermute(down_own, "tp", down)
    near = lax.all_gather(block, "sp_1")
    near, mirrored_queries = lax.optimization_barrier((near, mirrored_queries))
    own = lax.all_gather(near, "sp_0").reshape(-1, *block.shape)
    held_routes = lax.ppermute(routes, SP_TP, whole)
    own, held_routes, swapped_residual = lax.optimization_barrier((own, held_routes, residual_in))
    held_residual = lax.ppermute(swapped_residual, SP_TP, whole)
    other = lax.ppermute(own, "sp_2", [(0, 1), (1, 0)])
    attended = attend_rows(
        index.reshape(1), queries[:HALF], mirrored_queries, own, other
    )
    down_before, down_after, attended, held_residual = lax.optimization_barrier(
        (down_before, down_after, attended, held_residual)
    )
    half = down_own.shape[0] // 2
    across_low = lax.ppermute(down_before[:half], "tp", up)
    across_high = lax.ppermute(down_after[half:], "tp", down)
    partial = jnp.dot(
        attended.reshape(-1, attended.shape[2]), out_weight, preferred_element_type=jnp.float32
    ).astype(jnp.bfloat16)
    parts = lax.all_to_all(
        partial.reshape(head_devices, -1, partial.shape[1]), "tp", 0, 0, tiled=True
    )
    own_rows, top_count = routes.shape
    capacity = max(2, 3 * own_rows * top_count // (2 * seq_devices))
    ranked_routes = jnp.where(flipped, seq_devices - 1 - held_routes, held_routes)
    held_hidden, slots = dispatch(
        parts, held_residual, norm_gain, ranked_routes, seq_devices, capacity
    )
    down_across = jnp.concatenate([across_low, across_high])
    ranks = [
        [(i if 2 * t < head_devices else seq_devices - 1 - i) * head_devices + t for i in range(seq_devices)]
        for t in range(head_devices)
    ]
    incoming = lax.all_to_all(
        slots, SP_TP, 0, 0, axis_index_groups=ranks, tiled=True
    )
    incoming, held_hidden = lax.optimization_barrier((incoming, held_hidden))
    hidden_state = lax.ppermute(held_hidden, SP_TP, whole)
    rows_own = arrange(incoming, capacity)

    def units(rows):
        gate_value = jnp.dot(rows, expert_gate[0], preferred_element_type=jnp.float32)
        up_value = jnp.dot(rows, expert_up[0], preferred_element_type=jnp.float32)
        return (jax.nn.silu(gate_value) * up_value).astype(jnp.bfloat16)

    rows_before, rows_after = neighbours(rows_own)
    units_own = units(rows_own)
    rows_across = opposite(rows_before, rows_after)
    rows_across, hidden_state = lax.optimization_barrier((rows_across, hidden_state))
    units_from_before = lax.ppermute(units(rows_after), "tp", up)
    units_from_after = lax.ppermute(units(rows_before), "tp", down)
    across = [(i, (i + 2) % head_devices) for i in range(head_devices)]
    units_from_across = lax.ppermute(units(rows_across), "tp", across)
    summed = jnp.dot(units_own, down_own, preferred_element_type=jnp.float32)
    for got, weight in (
        (units_from_before, down_before),
        (units_from_after, down_after),
        (units_from_across, down_across),
    ):
        summed = summed + jnp.dot(got, weight, preferred_element_type=jnp.float32)
    returned = lax.all_to_all(spread(summed, capacity), SP, 0, 0, tiled=True)
    return combine(returned, hidden_state, routes, route_weight, capacity)


def solution(mesh):
    finer = Mesh(mesh.devices.reshape(8, 4, 2, mesh.shape["tp"]), ("sp_0", "sp_1", "sp_2", "tp"))
    in_specs = (
        P(SP, "tp"),
        P(SP, "tp"),
        P(SP, "tp"),
        P(SP_TP, None),
        P("tp", None),
        P(),
        P(SP_TP, None),
        P(SP_TP, None),
        P(SP, None, "tp"),
        P(SP, None, "tp"),
        P(SP, "tp", None),
    )
    out_specs = P(SP_TP, None)
    return jax.shard_map(layer, mesh=finer, in_specs=in_specs, out_specs=out_specs, check_vma=False)
```

```python
import functools
import math

import jax
import jax.numpy as jnp
from jax import lax
from jax.experimental import pallas as pl
from jax.experimental.pallas import tpu as pltpu
from jax.sharding import Mesh
from jax.sharding import PartitionSpec as P

SP = ("sp_0", "sp_1", "sp_2")
SP_TP = ("sp_0", "sp_1", "sp_2", "tp")
NORM_EPS = 1e-06
HEAD_SIZE = 64
NEG_FILL = -1e30
LOG2E = math.log2(math.e)
BLOCK = 256
HALF = 128
KEY_ROWS = 96
VALUE_ROWS = 64


SAFE_SCORE = 60.0
STEP = 1024
PAIRS = 2


def bf16_pieces(values):
    high = values.astype(jnp.bfloat16).astype(jnp.float32)
    rest = values - high
    middle = rest.astype(jnp.bfloat16).astype(jnp.float32)
    return [high, middle, rest - middle]


def prep_body(kv_ref, gate_ref, out_ref):
    kv = kv_ref[...].astype(jnp.float32).T
    keys = kv[:HEAD_SIZE]
    square = jnp.sum(keys * keys, axis=0, keepdims=True) * 1.02
    ones = jnp.ones_like(square)
    zeros = jnp.zeros_like(square)
    out_ref[...] = jnp.concatenate(
        [keys, *bf16_pieces(gate_ref[...])] + [ones] * 3 + [square] + [zeros] * 4 + [kv[HEAD_SIZE:]],
        axis=0,
    ).astype(jnp.bfloat16)


def prepare_keys(kv, gate_t):
    return pl.pallas_call(
        prep_body,
        out_shape=jax.ShapeDtypeStruct((KEY_ROWS + VALUE_ROWS, kv.shape[0]), jnp.bfloat16),
        name="prepare_keys",
    )(kv, gate_t)


def attend_body(index_ref, qa_ref, qb_ref, own_ref, other_ref, out_ref, qt_ref, max_ref, acc_ref, *, blocks, heads):
    columns = heads * HALF
    step = STEP
    own_index = index_ref[0]
    core = own_index % 2
    picked = 3 * heads
    row = lax.broadcasted_iota(jnp.int32, (picked, columns), 0)
    head = lax.broadcasted_iota(jnp.int32, (picked, columns), 1) // HALF
    picks = jnp.where(row % heads == head, -1.0, 0.0)
    largest_query = jnp.float32(0.0)
    mirror = blocks - 1 - own_index
    gates_at = slice(HEAD_SIZE, HEAD_SIZE + picked)
    gates_a = own_ref[own_index // 2, gates_at, :HALF].astype(jnp.float32)
    gates_b = other_ref[mirror // 2, gates_at, HALF:].astype(jnp.float32)
    for which, q_ref, gates in ((0, qa_ref, gates_a), (1, qb_ref, gates_b)):
        qt = (q_ref[...].astype(jnp.float32) * (HEAD_SIZE**-0.5)).T
        qt = jnp.concatenate(
            [qt[h * HEAD_SIZE : (h + 1) * HEAD_SIZE] for h in range(heads)], axis=1
        )
        largest_query = jnp.maximum(
            largest_query, jnp.max(jnp.sum(qt * qt, axis=0, keepdims=True))
        )
        pieces = [
            jnp.concatenate([gates[p + h : p + h + 1] for h in range(heads)], axis=1)
            for p in range(0, picked, heads)
        ]
        qt_ref[which] = jnp.concatenate(
            [qt, picks, *pieces, jnp.zeros((5, columns), jnp.float32)], axis=0
        ).astype(jnp.bfloat16)
    tail = slice(KEY_ROWS - 16, KEY_ROWS)
    squares = jnp.maximum(
        jnp.max(own_ref[:, tail].astype(jnp.float32), axis=0),
        jnp.max(other_ref[:, tail].astype(jnp.float32), axis=0),
    )
    largest_key = jnp.max(squares[11:12])
    bounded = largest_query * largest_key <= SAFE_SCORE**2
    acc_ref[...] = jnp.zeros(acc_ref.shape, jnp.float32)

    def operands(pair, count=1):
        tile = jnp.concatenate(
            [r[pair + n] for n in range(count) for r in (own_ref, other_ref)], axis=1
        )
        keys = tile[:KEY_ROWS].astype(jnp.float32).T.astype(jnp.bfloat16)
        values = jnp.concatenate(
            [tile[KEY_ROWS:], jnp.ones((16, tile.shape[1]), jnp.bfloat16)], axis=0
        )
        return keys, values

    def masked(scores, pair, first_row):
        k = lax.broadcasted_iota(jnp.int32, scores.shape, 0)
        t = lax.broadcasted_iota(jnp.int32, scores.shape, 1) % HALF
        start = jnp.where(k < BLOCK, core * BLOCK, (1 - core) * BLOCK - BLOCK)
        seen = pair * (2 * BLOCK) + start + k <= first_row + t
        return jnp.where(seen, scores, NEG_FILL)

    def plan(which):
        index = jnp.where(which == 0, own_index, blocks - 1 - own_index)
        return index // 2, index * BLOCK + which * HALF

    def plain(which, pair, first_row, count=1):
        keys, values = operands(pair, count)
        for at in range(0, columns, step):
            cols = slice(at, at + step)
            scores = jnp.dot(keys, qt_ref[which, :, cols], preferred_element_type=jnp.float32)
            if first_row is not None:
                scores = masked(scores, pair, first_row)
            weights = jnp.exp2(scores * LOG2E).astype(jnp.bfloat16)
            acc_ref[which, :, cols] += jnp.dot(values, weights, preferred_element_type=jnp.float32)

    def shifted(which, pair, first_row):
        keys, values = operands(pair)

        def chunk(c, carry):
            cols = pl.ds(pl.multiple_of(c * step, step), step)
            scores = jnp.dot(keys, qt_ref[which, :, cols], preferred_element_type=jnp.float32)
            scores = masked(scores, pair, first_row)
            before = max_ref[which, :, cols]
            now = jnp.maximum(before, jnp.max(scores, axis=0, keepdims=True))
            weights = jnp.exp2((scores - now) * LOG2E)
            rescale = jnp.exp2((before - now) * LOG2E)
            max_ref[which, :, cols] = now
            acc_ref[which, :, cols] = acc_ref[which, :, cols] * rescale + jnp.dot(
                values, weights.astype(jnp.bfloat16), preferred_element_type=jnp.float32
            )
            return carry

        lax.fori_loop(0, columns // step, chunk, 0)

    @pl.when(bounded)
    def _():
        def one(which, carry):
            last_pair, first_row = plan(which)

            def full(pair, inner):
                plain(which, pair, None)
                return inner

            def many(group, inner):
                plain(which, group * PAIRS, None, PAIRS)
                return inner

            groups = last_pair // PAIRS
            if PAIRS > 1:
                lax.fori_loop(0, groups, many, 0)
                lax.fori_loop(groups * PAIRS, last_pair, full, 0)
            else:
                lax.fori_loop(0, last_pair, full, 0)
            plain(which, last_pair, first_row)
            return carry

        lax.fori_loop(0, 2, one, 0)

    @pl.when(jnp.logical_not(bounded))
    def _():
        max_ref[...] = jnp.full(max_ref.shape, NEG_FILL, jnp.float32)

        def one(which, carry):
            last_pair, first_row = plan(which)

            def any_pair(pair, inner):
                shifted(which, pair, first_row)
                return inner

            lax.fori_loop(0, last_pair + 1, any_pair, 0)
            return carry

        lax.fori_loop(0, 2, one, 0)

    for which in range(2):
        acc = acc_ref[which]
        out = acc[:VALUE_ROWS] / acc[VALUE_ROWS : VALUE_ROWS + 1]
        out = jnp.concatenate([out[:, h * HALF : (h + 1) * HALF] for h in range(heads)], axis=0)
        out_ref[which] = out.T.astype(out_ref.dtype)


def attend_rows(index, qa, qb, own, other):
    heads = qa.shape[1] // HEAD_SIZE
    blocks = 2 * own.shape[0]
    columns = heads * HALF
    vmem = pl.BlockSpec(memory_space=pltpu.VMEM)
    return pl.pallas_call(
        functools.partial(attend_body, blocks=blocks, heads=heads),
        in_specs=[pl.BlockSpec(memory_space=pltpu.SMEM)] + [vmem] * 4,
        out_specs=vmem,
        out_shape=jax.ShapeDtypeStruct((2, *qa.shape), jnp.bfloat16),
        scratch_shapes=[
            pltpu.VMEM((2, KEY_ROWS, columns), jnp.bfloat16),
            pltpu.VMEM((2, 1, columns), jnp.float32),
            pltpu.VMEM((2, VALUE_ROWS + 16, columns), jnp.float32),
        ],
        compiler_params=pltpu.CompilerParams(vmem_limit_bytes=48 * 1024 * 1024),
        name="attend_rows",
    )(index, qa, qb, own, other)


def routing(routes_ref, experts):
    rows = routes_ref.shape[0]
    lanes = lax.broadcasted_iota(jnp.int32, (rows, experts), 1)
    first = (routes_ref[:, 0:1] == lanes).astype(jnp.float32)
    second = (routes_ref[:, 1:2] == lanes).astype(jnp.float32)
    named = first + second
    above = lax.broadcasted_iota(jnp.int32, (rows, rows), 1) < lax.broadcasted_iota(
        jnp.int32, (rows, rows), 0
    )
    earlier = jnp.dot(
        above.astype(jnp.bfloat16), named.astype(jnp.bfloat16), preferred_element_type=jnp.float32
    )
    return first, second, named, earlier


def spread_rows(tiles_ref, rows, slot, capacity):
    count, width = rows.shape
    per_row = width // 128
    for j in range(per_row):
        at = pl.ds(slot * per_row + j, count, stride=capacity * per_row)
        tiles_ref[at, :] = rows[:, j * 128 : (j + 1) * 128]


def joined_rows(tiles_ref, slot, capacity, count, width):
    per_row = width // 128
    return jnp.concatenate(
        [
            tiles_ref[pl.ds(slot * per_row + j, count, stride=capacity * per_row), :]
            for j in range(per_row)
        ],
        axis=1,
    )


def dispatch_body(parts_ref, residual_ref, gain_ref, routes_ref, hidden_ref, slots_ref, tiles_ref, *, capacity):
    mixed = jnp.sum(parts_ref[...].astype(jnp.float32), axis=0)
    hidden = residual_ref[...].astype(jnp.float32) + mixed
    hidden_ref[...] = hidden
    scale = lax.rsqrt(jnp.mean(hidden * hidden, axis=1, keepdims=True) + NORM_EPS)
    normed = (hidden * scale * gain_ref[...]).astype(jnp.bfloat16)
    experts = slots_ref.shape[0]
    _, _, named, earlier = routing(routes_ref, experts)
    for slot in range(capacity):
        chosen = jnp.where(earlier == slot, named, 0.0).T.astype(jnp.bfloat16)
        spread_rows(
            tiles_ref,
            jnp.dot(chosen, normed, preferred_element_type=jnp.float32),
            slot,
            capacity,
        )
    slots_ref[...] = tiles_ref[...].reshape(slots_ref.shape).astype(jnp.bfloat16)


def dispatch(parts, residual, gain, routes, experts, capacity):
    rows, width = residual.shape
    return pl.pallas_call(
        functools.partial(dispatch_body, capacity=capacity),
        out_shape=[
            jax.ShapeDtypeStruct((rows, width), jnp.float32),
            jax.ShapeDtypeStruct((experts, capacity * width // 128, 128), jnp.bfloat16),
        ],
        scratch_shapes=[pltpu.VMEM((experts * capacity * width // 128, 128), jnp.float32)],
        name="dispatch",
    )(parts, residual, gain.reshape(1, width), routes)


def arrange_body(arrived_ref, rows_ref, tiles_ref, *, capacity):
    count = arrived_ref.shape[0]
    tiles_ref[...] = arrived_ref[...].astype(jnp.float32).reshape(tiles_ref.shape)
    for slot in range(capacity):
        rows_ref[slot * count : (slot + 1) * count, :] = joined_rows(
            tiles_ref, slot, capacity, count, rows_ref.shape[1]
        ).astype(jnp.bfloat16)


def arrange(arrived, capacity):
    count, lines, lanes = arrived.shape
    return pl.pallas_call(
        functools.partial(arrange_body, capacity=capacity),
        out_shape=jax.ShapeDtypeStruct((capacity * count, lines * lanes // capacity), jnp.bfloat16),
        scratch_shapes=[pltpu.VMEM((count * lines, lanes), jnp.float32)],
        name="arrange",
    )(arrived)


def spread_body(rows_ref, leaving_ref, tiles_ref, *, capacity):
    count = leaving_ref.shape[0]
    for slot in range(capacity):
        rows = rows_ref[slot * count : (slot + 1) * count, :].astype(jnp.float32)
        spread_rows(tiles_ref, rows, slot, capacity)
    leaving_ref[...] = tiles_ref[...].reshape(leaving_ref.shape).astype(jnp.bfloat16)


def spread(rows, capacity):
    count, width = rows.shape[0] // capacity, rows.shape[1]
    lines = capacity * width // 128
    return pl.pallas_call(
        functools.partial(spread_body, capacity=capacity),
        out_shape=jax.ShapeDtypeStruct((count, lines, 128), jnp.bfloat16),
        scratch_shapes=[pltpu.VMEM((count * lines, 128), jnp.float32)],
        name="spread",
    )(rows)


def combine_body(returned_ref, hidden_ref, routes_ref, weight_ref, out_ref, tiles_ref, *, capacity):
    experts = returned_ref.shape[0]
    tiles_ref[...] = returned_ref[...].astype(jnp.float32).reshape(tiles_ref.shape)
    first, second, _, earlier = routing(routes_ref, experts)
    weight = first * weight_ref[:, 0:1] + second * weight_ref[:, 1:2]
    total = hidden_ref[...]
    for slot in range(capacity):
        rest = jnp.where(earlier == slot, weight, 0.0)
        rows = joined_rows(tiles_ref, slot, capacity, experts, out_ref.shape[1]).astype(jnp.bfloat16)
        for _ in range(3):
            piece = rest.astype(jnp.bfloat16)
            rest = rest - piece.astype(jnp.float32)
            total = total + jnp.dot(piece, rows, preferred_element_type=jnp.float32)
    out_ref[...] = total.astype(jnp.bfloat16)


def combine(returned, hidden, routes, route_weight, capacity):
    experts, lines, lanes = returned.shape
    return pl.pallas_call(
        functools.partial(combine_body, capacity=capacity),
        out_shape=jax.ShapeDtypeStruct(hidden.shape, jnp.bfloat16),
        scratch_shapes=[pltpu.VMEM((experts * lines, lanes), jnp.float32)],
        name="combine",
    )(returned, hidden, routes, route_weight)


def layer(
    queries,
    key_value_pairs,
    forget_gate_total,
    residual_in,
    out_weight,
    norm_gain,
    routes,
    route_weight,
    expert_gate,
    expert_up,
    expert_down,
):
    seq_devices = lax.axis_size(SP)
    head_devices = lax.axis_size("tp")
    index = lax.axis_index(SP).astype(jnp.int32)
    mirror = [(i, seq_devices - 1 - i) for i in range(seq_devices)]
    up = [(i, (i + 1) % head_devices) for i in range(head_devices)]
    down = [(i, (i - 1) % head_devices) for i in range(head_devices)]

    def neighbours(array):
        return lax.ppermute(array, "tp", up), lax.ppermute(array, "tp", down)

    def opposite(before, after):
        half = before.shape[0] // 2
        return jnp.concatenate(
            [lax.ppermute(before[:half], "tp", up), lax.ppermute(after[half:], "tp", down)], axis=0
        )

    whole = [
        (i * head_devices + t, (i if 2 * t < head_devices else seq_devices - 1 - i) * head_devices + t)
        for i in range(seq_devices)
        for t in range(head_devices)
    ]
    flipped = 2 * lax.axis_index("tp") >= head_devices
    block = prepare_keys(key_value_pairs, forget_gate_total.T)
    mirrored_queries = lax.ppermute(queries[HALF:], SP, mirror)
    down_own = expert_down[0]
    down_before = lax.ppermute(down_own, "tp", up)
    down_after = lax.ppermute(down_own, "tp", down)
    near = lax.all_gather(block, "sp_1")
    near, mirrored_queries = lax.optimization_barrier((near, mirrored_queries))
    own = lax.all_gather(near, "sp_0").reshape(-1, *block.shape)
    held_routes = lax.ppermute(routes, SP_TP, whole)
    own, held_routes, swapped_residual = lax.optimization_barrier((own, held_routes, residual_in))
    held_residual = lax.ppermute(swapped_residual, SP_TP, whole)
    other = lax.ppermute(own, "sp_2", [(0, 1), (1, 0)])
    attended = attend_rows(
        index.reshape(1), queries[:HALF], mirrored_queries, own, other
    )
    down_before, down_after, attended, held_residual = lax.optimization_barrier(
        (down_before, down_after, attended, held_residual)
    )
    half = down_own.shape[0] // 2
    across_low = lax.ppermute(down_before[:half], "tp", up)
    across_high = lax.ppermute(down_after[half:], "tp", down)
    partial = jnp.dot(
        attended.reshape(-1, attended.shape[2]), out_weight, preferred_element_type=jnp.float32
    ).astype(jnp.bfloat16)
    parts = lax.all_to_all(
        partial.reshape(head_devices, -1, partial.shape[1]), "tp", 0, 0, tiled=True
    )
    own_rows, top_count = routes.shape
    capacity = max(2, 3 * own_rows * top_count // (2 * seq_devices))
    ranked_routes = jnp.where(flipped, seq_devices - 1 - held_routes, held_routes)
    held_hidden, slots = dispatch(
        parts, held_residual, norm_gain, ranked_routes, seq_devices, capacity
    )
    down_across = jnp.concatenate([across_low, across_high])
    ranks = [
        [(i if 2 * t < head_devices else seq_devices - 1 - i) * head_devices + t for i in range(seq_devices)]
        for t in range(head_devices)
    ]
    incoming = lax.all_to_all(
        slots, SP_TP, 0, 0, axis_index_groups=ranks, tiled=True
    )
    incoming, held_hidden = lax.optimization_barrier((incoming, held_hidden))
    hidden_state = lax.ppermute(held_hidden, SP_TP, whole)
    rows_own = arrange(incoming, capacity)

    def units(rows):
        gate_value = jnp.dot(rows, expert_gate[0], preferred_element_type=jnp.float32)
        up_value = jnp.dot(rows, expert_up[0], preferred_element_type=jnp.float32)
        return (jax.nn.silu(gate_value) * up_value).astype(jnp.bfloat16)

    rows_before, rows_after = neighbours(rows_own)
    units_own = units(rows_own)
    rows_across = opposite(rows_before, rows_after)
    rows_across, hidden_state = lax.optimization_barrier((rows_across, hidden_state))
    units_from_before = lax.ppermute(units(rows_after), "tp", up)
    units_from_after = lax.ppermute(units(rows_before), "tp", down)
    across = [(i, (i + 2) % head_devices) for i in range(head_devices)]
    units_from_across = lax.ppermute(units(rows_across), "tp", across)
    summed = jnp.dot(units_own, down_own, preferred_element_type=jnp.float32)
    for got, weight in (
        (units_from_before, down_before),
        (units_from_after, down_after),
        (units_from_across, down_across),
    ):
        summed = summed + jnp.dot(got, weight, preferred_element_type=jnp.float32)
    returned = lax.all_to_all(spread(summed.astype(jnp.bfloat16), capacity), SP, 0, 0, tiled=True)
    return combine(returned, hidden_state, routes, route_weight, capacity)


def solution(mesh):
    finer = Mesh(mesh.devices.reshape(8, 4, 2, mesh.shape["tp"]), ("sp_0", "sp_1", "sp_2", "tp"))
    in_specs = (
        P(SP, "tp"),
        P(SP, "tp"),
        P(SP, "tp"),
        P(SP_TP, None),
        P("tp", None),
        P(),
        P(SP_TP, None),
        P(SP_TP, None),
        P(SP, None, "tp"),
        P(SP, None, "tp"),
        P(SP, "tp", None),
    )
    out_specs = P(SP_TP, None)
    return jax.shard_map(layer, mesh=finer, in_specs=in_specs, out_specs=out_specs, check_vma=False)
```
